128 devices in a mesh: sp: 32 (over z, y, core), tp: 4 (over x).
Axes of the slice: x: 4, y: 4, z: 4, core: 2. Of those that a mesh axis runs over, the one named last changes fastest.
Arguments:
- queries: bfloat16 [8192, 2048], P('sp', 'tp'), may hold values from -6 to 6
- key_value: bfloat16 [8192, 4, 128], P('sp', 'tp'), may hold values from -12 to 12
- break_bias: bfloat16 [8192, 32], P('sp', 'tp'), may hold values from -13 to 0
- stream: bfloat16 [8192, 2048], P(('sp', 'tp')), may hold values from -6 to 6
- out_proj: bfloat16 [2048, 2048], replicated, may hold values from -0.125 to 0.125
- ffn_gain: float32 [2048], replicated, may hold values from 0.1 to 1.9
- routes: int32 [8192, 4], P(('sp', 'tp')), may hold values from 0 to 127, all different within a row; in each aligned block of 64 rows (0 to 63, 64 to 127, ...) at most 4 rows name the same one
- route_score: float32 [8192, 4], P(('sp', 'tp')), may hold values from 0.05 to 1
- expert_gate: bfloat16 [128, 2048, 512], P(('sp', 'tp')), may hold values from -0.125 to 0.125
- expert_up: bfloat16 [128, 2048, 512], P(('sp', 'tp')), may hold values from -0.125 to 0.125
- expert_down: bfloat16 [128, 512, 2048], P(('sp', 'tp')), may hold values from -0.25 to 0.25
- shared_gate: bfloat16 [2048, 512], replicated, may hold values from -0.125 to 0.125
- shared_up: bfloat16 [2048, 512], replicated, may hold values from -0.125 to 0.125
- shared_down: bfloat16 [512, 2048], replicated, may hold values from -0.25 to 0.25
Outputs:
- layer_out: bfloat16 [8192, 2048], P(('sp', 'tp'))
The draws below stay inside these ranges and needn't reach their ends.
Inputs may be any that keep to these rules, and one draw needn't show every extreme that they name: `routes`: each row names 4 different experts. In each aligned block of 64 rows (the rows of one device) no expert is named by more than 4 rows, a bound that some block reaches.
All inputs are finite; a program needn't handle non-finite values.
Results may differ from the reference program's by a relative error of at most 0.015.
Values may be sent and summed in bfloat16 or wider, within the bound.
A program may use at most 128 MiB of HBM per device.

```python
import math
import jax
import jax.numpy as jnp
import numpy as np
from jax import lax

D = 2048
QUERY_HEADS = 32
KV_HEADS = 4
HD = 64
EFF = 512
SFF = 512
TOPK = 4
KEY_BLOCK = 1024
TOK_DEV = 256
SEQUENCE_TOKENS = 8192
ROWS_DEV = 64
EXPERTS = 128
CAP = 4


def draw_key_value(key, part):
    key_one, key_two, key_three = jax.random.split(jax.random.fold_in(key, 11), 3)
    block_total = SEQUENCE_TOKENS // TOK_DEV
    key_part = jax.random.normal(key_one, (SEQUENCE_TOKENS, KV_HEADS, HD), jnp.float32)
    noise_level = 1.5 * jax.random.normal(key_two, (block_total, 1, KV_HEADS, HD), jnp.float32)
    noise = jax.random.normal(key_three, (block_total, TOK_DEV, KV_HEADS, HD), jnp.float32)
    value_part = (noise_level + noise).reshape(SEQUENCE_TOKENS, KV_HEADS, HD)
    joined = jnp.concatenate([key_part, value_part], axis=2)
    return jnp.clip(joined, -12.0, 12.0).astype(jnp.bfloat16)


def draw_break_bias(key, part):
    key_vectors = jax.random.split(jax.random.fold_in(key, 23), 5)
    block_total = SEQUENCE_TOKENS // TOK_DEV
    fast_share = 0.5
    fast = jax.random.uniform(key_vectors[0], (QUERY_HEADS,), jnp.float32) < fast_share
    slow_level = -jnp.log(1.65 * SEQUENCE_TOKENS)
    noise_level = jnp.where(fast, jnp.log(1.0 / 40.0), slow_level)
    block_offset = jax.random.uniform(key_vectors[1], (block_total, 1, QUERY_HEADS), jnp.float32, -0.7, 0.7)
    block_offset = jnp.broadcast_to(block_offset, (block_total, TOK_DEV, QUERY_HEADS)).reshape(SEQUENCE_TOKENS, QUERY_HEADS)
    coarse_noise = jax.random.uniform(key_vectors[2], (SEQUENCE_TOKENS, QUERY_HEADS), jnp.float32, -0.5, 0.5)
    sudden_spike = jax.random.uniform(key_vectors[3], (SEQUENCE_TOKENS, QUERY_HEADS), jnp.float32) < 2.0 / SEQUENCE_TOKENS
    spike_value = jax.random.uniform(key_vectors[4], (SEQUENCE_TOKENS, QUERY_HEADS), jnp.float32, -1.4, 0.0)
    offset_rows = jnp.where(sudden_spike, spike_value, noise_level[None, :] + block_offset + coarse_noise)
    return jnp.clip(offset_rows, -13.0, 0.0).astype(jnp.bfloat16)


def block_levels(key, dims, shards, low, high):
    def one(dim, blocks):
        heights = jax.random.uniform(jax.random.fold_in(jax.random.fold_in(key, 6), dim), (blocks,), jnp.float32, low / len(shards), high / len(shards))
        return jnp.repeat(jnp.exp(heights), dims[dim] // blocks).reshape((-1,) + (1,) * (len(dims) - dim - 1))

    gain = one(*shards[0])
    for cut in shards[1:]:
        gain = gain * one(*cut)
    return gain


def assign_block(key, own, number, rows, number_of, top, bound, slope):
    order = jax.random.permutation(key, number_of)
    crowded, common = portions_of(number_of, rows * top, bound, slope, True), portions_of(number_of, rows * top, bound, slope, False)
    places = jnp.arange(number_of)

    def named(lengths, turn):
        used = int((lengths > 0).sum())
        fixed = max(1, used // 4)
        moved = fixed + (places - fixed + turn * (used - fixed)) % max(1, number_of - fixed)
        return jnp.zeros((number_of,), jnp.int32).at[order[jnp.where(places < fixed, places, moved)]].set(jnp.asarray(lengths, jnp.int32))

    lengths = jnp.where(number % 4 == 0, named(crowded, number // 4), named(common, number - number // 4 - 1))
    mixed = jax.random.permutation(jax.random.fold_in(own, 3), number_of)
    giver, sink = mixed[0:number_of // 2 * 2:2], mixed[1:number_of // 2 * 2:2]
    room = jnp.minimum(lengths[giver] - 1, bound - lengths[sink]) // 2
    room = jnp.where((giver == order[0]) | (sink == order[0]) | (lengths[sink] == 0), 0, jnp.maximum(room, 0))
    moved = jax.random.randint(jax.random.fold_in(own, 4), (number_of // 2,), 0, 1 << 20) % (room + 1)
    lengths = lengths.at[giver].add(-moved).at[sink].add(moved)
    items = jnp.searchsorted(jnp.cumsum(lengths), jnp.arange(rows * top), side="right").astype(jnp.int32)
    grid = items.reshape(top, rows).T
    grid = grid[jax.random.permutation(jax.random.fold_in(own, 1), rows)]
    turn = jax.random.randint(jax.random.fold_in(own, 2), (rows, 1), 0, top)
    return jnp.take_along_axis(grid, (jnp.arange(top)[None, :] + turn) % top, axis=1)


def portions_of(count, total, limit, skew, full):
    portions = [(1 << 20) // math.isqrt(standing ** skew) + 1 for standing in range(1, count + 1)]
    largest = limit if full else min(limit, max(-(-total // count), total * portions[0] // sum(portions)))
    least = 1 if total - largest >= count - 1 else 0
    holding, surplus = [largest] + [least] * (count - 1), total - largest - least * (count - 1)
    while surplus > 0:
        candidates = [i for i in range(1, count) if holding[i] < largest] or [i for i in range(1, count) if holding[i] < limit]
        whole, remaining = sum([portions[i] for i in candidates]), surplus
        for i in candidates:
            addition = min(limit - holding[i], max(1, remaining * portions[i] // whole), surplus)
            holding[i] = holding[i] + addition
            surplus = surplus - addition
    return np.array(holding)


def bell_draw(own_key, shape, spread, limit, pieces=(), held_as=jnp.bfloat16):
    gain = block_levels(own_key, shape, pieces, -0.22, 0.18) if pieces else 1.0
    result = jax.random.normal(own_key, shape, jnp.float32) * spread * gain
    return jnp.minimum(jnp.maximum(result, -limit), limit).astype(held_as)


def setup_inputs(seed: int = 0) -> dict:
    keys = jax.random.split(jax.random.key(seed), 15)
    queries = bell_draw(keys[0], (SEQUENCE_TOKENS, QUERY_HEADS * HD), 1.0, 6.0, ((0, 32), (1, 4)))
    key_value = draw_key_value(jax.random.fold_in(keys[14], 71), 0)
    break_bias = draw_break_bias(jax.random.fold_in(keys[14], 71), 0)
    stream = bell_draw(keys[3], (SEQUENCE_TOKENS, D), 1.0, 6.0, ((0, 128),))
    out_proj = bell_draw(keys[4], (QUERY_HEADS * HD, D), (QUERY_HEADS * HD) ** -0.5, 0.125)
    ffn_gain = jnp.clip(1.0 + 0.18 * jax.random.normal(keys[5], (D,), jnp.float32), 0.1, 1.9)
    routes_keys = jax.random.split(jax.random.fold_in(keys[6], 1), SEQUENCE_TOKENS // ROWS_DEV)
    routes_turns = jax.random.permutation(jax.random.fold_in(keys[6], 3), SEQUENCE_TOKENS // ROWS_DEV)
    routes = jax.vmap(lambda own, number: assign_block(jax.random.fold_in(keys[6], 2), own, number, ROWS_DEV, EXPERTS, TOPK, CAP, 2))(routes_keys, routes_turns).reshape((SEQUENCE_TOKENS, TOPK))
    route_score = jnp.clip(jnp.exp(math.log(1.0) - 2.9957323 * jax.random.uniform(keys[7], (SEQUENCE_TOKENS, TOPK), jnp.float32) ** block_levels(keys[7], (SEQUENCE_TOKENS, TOPK), ((0, 128),), -0.2, 0.2)), 0.05, 1.0)
    expert_gate = bell_draw(keys[8], (EXPERTS, D, EFF), D ** -0.5, 0.125, ((0, 128),))
    expert_up = bell_draw(keys[9], (EXPERTS, D, EFF), D ** -0.5, 0.125, ((0, 128),))
    expert_down = bell_draw(keys[10], (EXPERTS, EFF, D), EFF ** -0.5, 0.25, ((0, 128),))
    shared_gate = bell_draw(keys[11], (D, SFF), D ** -0.5, 0.125)
    shared_up = bell_draw(keys[12], (D, SFF), D ** -0.5, 0.125)
    shared_down = bell_draw(keys[13], (SFF, D), SFF ** -0.5, 0.25)
    return {"queries": queries, "key_value": key_value, "break_bias": break_bias, "stream": stream, "out_proj": out_proj, "ffn_gain": ffn_gain, "routes": routes, "route_score": route_score, "expert_gate": expert_gate, "expert_up": expert_up, "expert_down": expert_down, "shared_gate": shared_gate, "shared_up": shared_up, "shared_down": shared_down}


def pad_front(values, count):
    filler = jnp.zeros((count,) + values.shape[1:], values.dtype)
    return jnp.concatenate([filler, values], axis=0)

def stick_sweep(query_block, key_value, break_bias, query_start, key_block):
    query_rows, kv_heads, group_size, head_size = query_block.shape
    scale = head_size ** (-0.5)
    query_pos = query_start + jnp.arange(query_rows, dtype=jnp.int32)
    query_end = query_start + query_rows
    block_count = (query_end + key_block - 1) // key_block
    query_wide = query_block.astype(jnp.float32)

    def one_block(block_index, carry):
        output, carried = carry
        key_start = (query_end - (block_index + 1) * key_block).astype(jnp.int32)
        rows_here = lax.dynamic_slice_in_dim(key_value, key_start + key_block, key_block, 0)
        shift_here = lax.dynamic_slice_in_dim(break_bias, key_start + key_block, key_block, 0).astype(jnp.float32)
        key_part = rows_here[..., :head_size].astype(jnp.float32)
        value_part = rows_here[..., head_size:].astype(jnp.float32)
        logits = jnp.einsum('qhgd,khd->hgqk', query_wide, key_part) * scale
        logits = logits + jnp.transpose(shift_here, (1, 2, 0))[:, :, None, :]
        key_pos = key_start + jnp.arange(key_block, dtype=jnp.int32)
        valid = (key_pos[None, :] < query_pos[:, None]) & (key_pos[None, :] >= 0)
        log_stay = jnp.where(valid, jax.nn.log_sigmoid(-logits), 0.0)
        beyond = lax.cumsum(log_stay, axis=3, reverse=True) - log_stay + carried[..., None]
        weight = jnp.where(valid, jnp.exp(jax.nn.log_sigmoid(logits) + beyond), 0.0)
        weight = lax.optimization_barrier(weight.astype(jnp.bfloat16)).astype(jnp.float32)
        output = output + jnp.einsum('hgqk,khd->qhgd', weight, value_part)
        return (output, carried + lax.optimization_barrier(jnp.sum(log_stay, axis=3)))
    start_state = (jnp.zeros((query_rows, kv_heads, group_size, head_size), jnp.float32), jnp.zeros((kv_heads, group_size, query_rows), jnp.float32))
    output, _ = lax.fori_loop(0, block_count, one_block, start_state)
    return output.astype(jnp.bfloat16).reshape(query_rows, kv_heads * group_size * head_size)

def rms_scale(resid, ffn_gain):
    wide = resid.astype(jnp.float32)
    factor = lax.rsqrt(lax.optimization_barrier(jnp.mean(wide * wide, axis=-1, keepdims=True)) + 1e-06)
    return (wide * factor * ffn_gain).astype(jnp.bfloat16)

def reference(queries, key_value, break_bias, stream, out_proj, ffn_gain, routes, route_score, expert_gate, expert_up, expert_down, shared_gate, shared_up, shared_down):
    group_size = QUERY_HEADS // KV_HEADS
    query_grid = queries.reshape(SEQUENCE_TOKENS // TOK_DEV, TOK_DEV, KV_HEADS, group_size, HD)
    padded_kv = pad_front(key_value, KEY_BLOCK)
    padded_bias = pad_front(break_bias.reshape(SEQUENCE_TOKENS, KV_HEADS, group_size), KEY_BLOCK)
    starts = jnp.arange(SEQUENCE_TOKENS // TOK_DEV, dtype=jnp.int32) * TOK_DEV

    def sweep_block(packed):
        return stick_sweep(packed[0], padded_kv, padded_bias, packed[1], KEY_BLOCK)
    attended = lax.map(sweep_block, (query_grid, starts)).reshape(SEQUENCE_TOKENS, QUERY_HEADS * HD)
    mixed = jnp.dot(attended, out_proj, preferred_element_type=jnp.float32)
    resid = (stream.astype(jnp.float32) + mixed).astype(jnp.bfloat16)
    normed = rms_scale(resid, ffn_gain)
    gates = 2.5 * route_score / lax.optimization_barrier(jnp.sum(route_score, axis=1, keepdims=True))
    flat_expert = routes.reshape(-1).astype(jnp.int32)
    flat_row = jnp.repeat(jnp.arange(SEQUENCE_TOKENS, dtype=jnp.int32), TOPK)
    onehot = (flat_expert[:, None] == jnp.arange(EXPERTS, dtype=jnp.int32)[None, :]).astype(jnp.int32)
    rank = lax.optimization_barrier(jnp.sum((jnp.cumsum(onehot, axis=0) - onehot) * onehot, axis=1)).astype(jnp.int32)
    slot_count = SEQUENCE_TOKENS // ROWS_DEV * CAP
    row_table = jnp.full((EXPERTS, slot_count), SEQUENCE_TOKENS, jnp.int32).at[flat_expert, rank].set(flat_row)
    gate_table = jnp.zeros((EXPERTS, slot_count), jnp.float32).at[flat_expert, rank].set(gates.reshape(-1))
    normed_pad = jnp.concatenate([normed, jnp.zeros((1, D), normed.dtype)], axis=0)

    def expert_step(total, packed):
        row_ids, gate_ids, w_gate, w_up, w_down = packed
        chosen = normed_pad[row_ids]
        gate_part = jnp.dot(chosen, w_gate, preferred_element_type=jnp.float32)
        up_part = jnp.dot(chosen, w_up, preferred_element_type=jnp.float32)
        inner = (jax.nn.silu(gate_part) * up_part).astype(jnp.bfloat16)
        done = jnp.dot(inner, w_down, preferred_element_type=jnp.float32).astype(jnp.bfloat16)
        return (total.at[row_ids].add(gate_ids[:, None] * done.astype(jnp.float32)), None)
    routed, _ = lax.scan(expert_step, jnp.zeros((SEQUENCE_TOKENS + 1, D), jnp.float32), (row_table, gate_table, expert_gate, expert_up, expert_down))
    shared_inner = (jax.nn.silu(jnp.dot(normed, shared_gate, preferred_element_type=jnp.float32)) * jnp.dot(normed, shared_up, preferred_element_type=jnp.float32)).astype(jnp.bfloat16)
    shared_out = jnp.dot(shared_inner, shared_down, preferred_element_type=jnp.float32)
    return (resid.astype(jnp.float32) + shared_out + routed[:SEQUENCE_TOKENS]).astype(jnp.bfloat16)
```

```python
import functools

import jax
import jax.numpy as jnp
import numpy as np
from jax import lax
from jax.experimental import pallas as pl
from jax.experimental.pallas import tpu as pltpu
from jax.sharding import PartitionSpec as P

GROUP = 8
LOG2E = 1.4426950408889634


def schedule(blocks, tiles, group):
    half = blocks // 2
    rows = []
    give = []
    for i in range(half):
        best = min(range(0, tiles // 2 + 1), key=lambda n: max(tiles * (i + 1) + n * (blocks - i), (tiles - n) * (blocks - i)))
        give.append(best)
    for i in range(blocks):
        n = give[min(i, blocks - 1 - i)]
        if i < half:
            slots = [(s, i) for s in range(tiles)] + [(tiles + s, blocks - 1 - i) for s in range(n)]
        else:
            slots = [(s, i) for s in range(n, tiles)]
        diag = [(s, q) for s, q in slots]
        main = []
        depth = max(q for _, q in slots)
        for back in range(1, depth + 1):
            for s, q in slots:
                if q - back >= 0:
                    main.append((s, q - back))
        rows.append((diag, main))
    spare = tiles + tiles // 2
    ld = max(-(-len(d) // group) for d, _ in rows)
    lm = max(-(-len(m) // group) for _, m in rows)
    table = np.zeros((blocks, 2 + 2 * group * (ld + lm)), np.int32)
    for i, (diag, main) in enumerate(rows):
        nd, nm = -(-len(diag) // group), -(-len(main) // group)
        diag = diag + [(spare, 0)] * (group * ld - len(diag))
        main = main + [(spare, 0)] * (group * lm - len(main))
        table[i, 0], table[i, 1] = nd, nm
        table[i, 2:] = np.array(diag + main).reshape(-1)
    return table, np.array(give), ld, lm


def attend_kernel(group, ld, tab, q_ref, kv_ref, tri_ref, out_ref, qs, acc, carry):
    nt = out_ref.shape[0] // 32
    f32, bf16 = jnp.float32, jnp.bfloat16
    head_lane = lax.broadcasted_iota(jnp.int32, (32, 16), 1)
    c_hi = float(np.asarray(LOG2E, jnp.bfloat16))
    c_lo = float(np.float32(LOG2E - c_hi))

    def build(s, _):
        q = q_ref[pl.ds(s * 32, 32), :].astype(f32) * (0.125 * LOG2E)
        hi = q.astype(bf16)
        lo = (q - hi.astype(f32)).astype(bf16)
        for h in range(8):
            tail = jnp.where(head_lane == h, c_hi, jnp.where(head_lane == h + 8, c_lo, 0.0)).astype(bf16)
            qs[s, pl.ds(h * 32, 32), :] = jnp.concatenate([hi[:, 64 * h:64 * h + 64], lo[:, 64 * h:64 * h + 64], tail], axis=1)
        return 0

    lax.fori_loop(0, nt, build, 0)
    qs[nt] = jnp.zeros_like(qs[nt])
    acc[...] = jnp.zeros_like(acc)
    carry[...] = jnp.zeros_like(carry)
    lane = lax.broadcasted_iota(jnp.int32, (128, 128), 1)

    def step(base, masked):
        for g in range(group):
            slot = tab[base + 2 * g]
            chunk = tab[base + 2 * g + 1]
            key = jnp.concatenate([kv_ref[chunk, 0:64, :], kv_ref[chunk, 0:80, :]], axis=0)
            z = jnp.dot(qs[slot], key, preferred_element_type=f32)
            if masked:
                row = lax.broadcasted_iota(jnp.int32, (256, 256), 0) % 32 + (slot % 8) * 32
                col = lax.broadcasted_iota(jnp.int32, (256, 256), 1)
                z = jnp.where(col < row, z, -1e30)
            sp = jnp.maximum(z, lax.log2(1.0 + jnp.exp2(jnp.minimum(z, 126.0))))
            u = z - sp
            sums = jnp.dot(sp.astype(bf16), tri_ref[...], preferred_element_type=f32)
            before = carry[slot]
            w = jnp.exp2(u - sums[:, :256] - jnp.concatenate([before, before], axis=1)).astype(bf16)
            carry[slot] = before + sums[:, 256:]
            vx = kv_ref[chunk, 80:144, :]
            v = jnp.concatenate([vx[:, :128], vx[:, 128:]], axis=0)
            zero = jnp.zeros_like(v)
            both = jnp.concatenate([jnp.where(lane < 64, v, zero), jnp.where(lane < 64, zero, v)], axis=0)
            acc[slot] += jnp.dot(w, both, preferred_element_type=f32)

    def diag_step(j, _):
        step(2 + 2 * group * j, True)
        return 0

    def main_step(j, _):
        step(2 + 2 * group * (ld + j), False)
        return 0

    lax.fori_loop(0, tab[0], diag_step, 0)
    lax.fori_loop(0, tab[1], main_step, 0)

    def finish(s, _):
        for p in range(4):
            pair = []
            for h in (2 * p, 2 * p + 1):
                a = acc[s, pl.ds(h * 32, 32), :]
                pair.append(a[:, :64] + a[:, 64:])
            out_ref[pl.ds(s * 32, 32), pl.ds(128 * p, 128)] = jnp.concatenate(pair, axis=1).astype(bf16)
        return 0

    lax.fori_loop(0, nt, finish, 0)


def triangle():
    t = np.zeros((256, 384), np.float32)
    t[:, :256] = np.tril(np.ones((256, 256)), -1)
    t[:, 256:] = 1.0
    return t


def attend(tab, q_all, kv, group, ld):
    nt = q_all.shape[0] // 32
    vm = pl.BlockSpec(memory_space=pltpu.VMEM)
    return pl.pallas_call(
        functools.partial(attend_kernel, group, ld),
        out_shape=jax.ShapeDtypeStruct(q_all.shape, jnp.bfloat16),
        in_specs=[pl.BlockSpec(memory_space=pltpu.SMEM), vm, vm, vm],
        out_specs=vm,
        scratch_shapes=[pltpu.VMEM((nt + 1, 256, 144), jnp.bfloat16), pltpu.VMEM((nt + 1, 256, 128), jnp.float32), pltpu.VMEM((nt + 1, 256, 128), jnp.float32)],
        compiler_params=pltpu.CompilerParams(vmem_limit_bytes=48 * 1024 * 1024),
        name="attend",
    )(tab, q_all, kv, jnp.asarray(triangle(), jnp.bfloat16))


def pack_kv(key_value, bias):
    kt = key_value[:, :64].T
    b = bias.T
    v = key_value[:, 64:]
    left = jnp.concatenate([v[0:64], v[128:192]], axis=1)
    right = jnp.concatenate([v[64:128], v[192:256]], axis=1)
    return jnp.concatenate([kt, b, b, jnp.concatenate([left, right], axis=1)], axis=0)


def from_everyone(array, axis):
    copies = jnp.broadcast_to(array, (lax.axis_size(axis), *array.shape))
    return lax.all_to_all(copies, axis, split_axis=0, concat_axis=0, tiled=True)


def expert_rows(arrived, w_gate, w_up, w_down):
    gate_part = jnp.einsum("snd,df->snf", arrived, w_gate, preferred_element_type=jnp.float32)
    up_part = jnp.einsum("snd,df->snf", arrived, w_up, preferred_element_type=jnp.float32)
    inner = (jax.nn.silu(gate_part) * up_part).astype(jnp.bfloat16)
    return jnp.einsum("snf,fd->snd", inner, w_down, preferred_element_type=jnp.float32).astype(
        jnp.bfloat16
    )


def body(
    queries,
    key_value,
    break_bias,
    stream,
    out_proj,
    ffn_gain,
    routes,
    route_score,
    expert_gate,
    expert_up,
    expert_down,
    shared_gate,
    shared_up,
    shared_down,
):
    table, give, diag_groups, _ = schedule(lax.axis_size("sp"), queries.shape[0] // 32, GROUP)
    blocks = lax.axis_size("sp")
    half = queries.shape[0] // 2
    me = lax.axis_index("sp")
    kv = from_everyone(pack_kv(key_value[:, 0, :], break_bias), "sp")
    kv = kv.reshape(blocks, -1, kv.shape[-1])
    down = [(h, blocks - 1 - h) for h in range(blocks // 2, blocks)]
    up = [(b, a) for a, b in down]
    theirs = lax.ppermute(queries[:half], "sp", down)
    tab = lax.dynamic_index_in_dim(jnp.asarray(table), me, 0, keepdims=False)
    done_rows = attend(tab, jnp.concatenate([queries, theirs], axis=0), kv, GROUP, diag_groups)
    back = lax.ppermute(done_rows[2 * half :], "sp", up)
    given = jnp.asarray(give, jnp.int32)[jnp.minimum(me, blocks - 1 - me)] * 32
    mine = (me < blocks // 2) | (jnp.arange(half)[:, None] >= given)
    attended = jnp.concatenate(
        [jnp.where(mine, done_rows[:half], back), done_rows[half : 2 * half]], axis=0
    )
    token_heads = lax.all_to_all(attended, "tp", split_axis=0, concat_axis=1, tiled=True)
    mixed = jnp.dot(token_heads, out_proj, preferred_element_type=jnp.float32)
    resid = (stream.astype(jnp.float32) + mixed).astype(jnp.bfloat16)
    wide = resid.astype(jnp.float32)
    factor = lax.rsqrt(jnp.mean(wide * wide, axis=-1, keepdims=True) + 1e-06)
    normed = (wide * factor * ffn_gain).astype(jnp.bfloat16)
    gates = 2.5 * route_score / jnp.sum(route_score, axis=1, keepdims=True)
    row_count = resid.shape[0]
    top_count = routes.shape[1]
    shard_sp = lax.axis_size("sp")
    shard_tp = lax.axis_size("tp")
    expert_count = shard_sp * shard_tp
    capacity = 2 * row_count * top_count // expert_count
    width = resid.shape[1]
    flat_expert = routes.reshape(-1)
    onehot = (flat_expert[:, None] == jnp.arange(expert_count, dtype=jnp.int32)[None, :]).astype(
        jnp.int32
    )
    rank = jnp.sum((jnp.cumsum(onehot, axis=0) - onehot) * onehot, axis=1)
    slot_ids = (flat_expert * capacity + rank).reshape(row_count, top_count)
    slot_grid = jnp.arange(expert_count * capacity, dtype=jnp.int32)
    pick = jnp.any(slot_ids[:, :, None] == slot_grid[None, None, :], axis=1).astype(jnp.bfloat16)
    outgoing = jnp.einsum("rs,rd->sd", pick, normed, preferred_element_type=jnp.float32).astype(
        jnp.bfloat16
    )
    outgoing = outgoing.reshape(expert_count, capacity, width)
    done = expert_rows(
        lax.all_to_all(outgoing, ("sp", "tp"), split_axis=0, concat_axis=0, tiled=True),
        expert_gate[0],
        expert_up[0],
        expert_down[0],
    )
    returned = lax.all_to_all(done, ("sp", "tp"), split_axis=0, concat_axis=0, tiled=True)
    flat_back = returned.reshape(expert_count * capacity, width)
    picked_rows = flat_back[slot_ids.reshape(-1)].reshape(row_count, top_count, width)
    routed = jnp.einsum("rk,rkd->rd", gates, picked_rows.astype(jnp.float32))
    shared_inner = (
        jax.nn.silu(jnp.dot(normed, shared_gate, preferred_element_type=jnp.float32))
        * jnp.dot(normed, shared_up, preferred_element_type=jnp.float32)
    ).astype(jnp.bfloat16)
    shared_out = jnp.dot(shared_inner, shared_down, preferred_element_type=jnp.float32)
    return (wide + shared_out + routed).astype(jnp.bfloat16)


def solution(mesh):
    return jax.shard_map(
        body,
        mesh=mesh,
        in_specs=(
            P("sp", "tp"),
            P("sp", "tp", None),
            P("sp", "tp"),
            P(("sp", "tp"), None),
            P(),
            P(),
            P(("sp", "tp"), None),
            P(("sp", "tp"), None),
            P(("sp", "tp"), None, None),
            P(("sp", "tp"), None, None),
            P(("sp", "tp"), None, None),
            P(),
            P(),
            P(),
        ),
        out_specs=P(("sp", "tp"), None),
        check_vma=False,
    )
```

```python
import functools

import jax
import jax.numpy as jnp
import numpy as np
from jax import lax
from jax.experimental import pallas as pl
from jax.experimental.pallas import tpu as pltpu
from jax.sharding import PartitionSpec as P

GROUP = 8
LOG2E = 1.4426950408889634


def schedule(blocks, tiles, group):
    half = blocks // 2
    rows = []
    give = []
    for i in range(half):
        best = min(range(0, tiles // 2 + 1), key=lambda n: max(tiles * (i + 1) + n * (blocks - i), (tiles - n) * (blocks - i)))
        give.append(best)
    for i in range(blocks):
        n = give[min(i, blocks - 1 - i)]
        if i < half:
            slots = [(s, i) for s in range(tiles)] + [(tiles + s, blocks - 1 - i) for s in range(n)]
        else:
            slots = [(s, i) for s in range(n, tiles)]
        diag = [(s, q) for s, q in slots]
        main = []
        depth = max(q for _, q in slots)
        for back in range(1, depth + 1):
            for s, q in slots:
                if q - back >= 0:
                    main.append((s, q - back))
        rows.append((diag, main))
    spare = tiles + tiles // 2
    ld = max(-(-len(d) // group) for d, _ in rows)
    lm = max(-(-len(m) // group) for _, m in rows)
    table = np.zeros((blocks, 2 + 2 * group * (ld + lm)), np.int32)
    for i, (diag, main) in enumerate(rows):
        nd, nm = -(-len(diag) // group), -(-len(main) // group)
        diag = diag + [(spare, 0)] * (group * ld - len(diag))
        main = main + [(spare, 0)] * (group * lm - len(main))
        table[i, 0], table[i, 1] = nd, nm
        table[i, 2:] = np.array(diag + main).reshape(-1)
    return table, np.array(give), ld, lm


def attend_kernel(group, ld, tab, q_ref, kv_ref, tri_ref, out_ref, qs, acc, carry):
    nt = out_ref.shape[0] // 32
    f32, bf16 = jnp.float32, jnp.bfloat16
    head_lane = lax.broadcasted_iota(jnp.int32, (32, 16), 1)
    c_hi = float(np.asarray(LOG2E, jnp.bfloat16))
    c_lo = float(np.float32(LOG2E - c_hi))

    def build(s, _):
        q = q_ref[pl.ds(s * 32, 32), :].astype(f32) * (0.125 * LOG2E)
        hi = q.astype(bf16)
        lo = (q - hi.astype(f32)).astype(bf16)
        for h in range(8):
            tail = jnp.where(head_lane == h, c_hi, jnp.where(head_lane == h + 8, c_lo, 0.0)).astype(bf16)
            qs[s, pl.ds(h * 32, 32), :] = jnp.concatenate([hi[:, 64 * h:64 * h + 64], lo[:, 64 * h:64 * h + 64], tail], axis=1)
        return 0

    lax.fori_loop(0, nt, build, 0)
    qs[nt] = jnp.zeros_like(qs[nt])
    acc[...] = jnp.zeros_like(acc)
    carry[...] = jnp.zeros_like(carry)
    lane = lax.broadcasted_iota(jnp.int32, (128, 128), 1)

    def step(base, masked):
        for g in range(group):
            slot = tab[base + 2 * g]
            chunk = tab[base + 2 * g + 1]
            key = jnp.concatenate([kv_ref[chunk, 0:64, :], kv_ref[chunk, 0:80, :]], axis=0)
            z = jnp.dot(qs[slot], key, preferred_element_type=f32)
            if masked:
                row = lax.broadcasted_iota(jnp.int32, (256, 256), 0) % 32 + (slot % 8) * 32
                col = lax.broadcasted_iota(jnp.int32, (256, 256), 1)
                z = jnp.where(col < row, z, -1e30)
            sp = jnp.maximum(z, lax.log2(1.0 + jnp.exp2(jnp.minimum(z, 126.0))))
            u = z - sp
            sums = jnp.dot(sp.astype(bf16), tri_ref[...], preferred_element_type=f32)
            before = carry[slot]
            w = jnp.exp2(u - sums[:, :256] - jnp.concatenate([before, before], axis=1)).astype(bf16)
            carry[slot] = before + sums[:, 256:]
            vx = kv_ref[chunk, 80:144, :]
            v = jnp.concatenate([vx[:, :128], vx[:, 128:]], axis=0)
            zero = jnp.zeros_like(v)
            both = jnp.concatenate([jnp.where(lane < 64, v, zero), jnp.where(lane < 64, zero, v)], axis=0)
            acc[slot] += jnp.dot(w, both, preferred_element_type=f32)

    def diag_step(j, _):
        step(2 + 2 * group * j, True)
        return 0

    def main_step(j, _):
        step(2 + 2 * group * (ld + j), False)
        return 0

    lax.fori_loop(0, tab[0], diag_step, 0)
    lax.fori_loop(0, tab[1], main_step, 0)

    def finish(s, _):
        for p in range(4):
            pair = []
            for h in (2 * p, 2 * p + 1):
                a = acc[s, pl.ds(h * 32, 32), :]
                pair.append(a[:, :64] + a[:, 64:])
            out_ref[pl.ds(s * 32, 32), pl.ds(128 * p, 128)] = jnp.concatenate(pair, axis=1).astype(bf16)
        return 0

    lax.fori_loop(0, nt, finish, 0)


def triangle():
    t = np.zeros((256, 384), np.float32)
    t[:, :256] = np.tril(np.ones((256, 256)), -1)
    t[:, 256:] = 1.0
    return t


def attend(tab, q_all, kv, group, ld):
    nt = q_all.shape[0] // 32
    vm = pl.BlockSpec(memory_space=pltpu.VMEM)
    return pl.pallas_call(
        functools.partial(attend_kernel, group, ld),
        out_shape=jax.ShapeDtypeStruct(q_all.shape, jnp.bfloat16),
        in_specs=[pl.BlockSpec(memory_space=pltpu.SMEM), vm, vm, vm],
        out_specs=vm,
        scratch_shapes=[pltpu.VMEM((nt + 1, 256, 144), jnp.bfloat16), pltpu.VMEM((nt + 1, 256, 128), jnp.float32), pltpu.VMEM((nt + 1, 256, 128), jnp.float32)],
        compiler_params=pltpu.CompilerParams(vmem_limit_bytes=48 * 1024 * 1024),
        name="attend",
    )(tab, q_all, kv, jnp.asarray(triangle(), jnp.bfloat16))


MESH = pl.DeviceIdType.MESH
VM = pl.BlockSpec(memory_space=pltpu.VMEM)


def place():
    sp, x = lax.axis_index("sp"), lax.axis_index("tp")
    return sp // 8, (sp // 2) % 4, sp % 2, x


def given_tiles(sp, thresholds):
    low = jnp.minimum(sp, 31 - sp)
    n = jnp.int32(0)
    for t in thresholds:
        n = n + jnp.where(low < t, 1, 0)
    return n


def pack_kernel(kv_ref, bias_ref, out_ref):
    f32, bf16 = jnp.float32, jnp.bfloat16
    kv = kv_ref[...].astype(f32)
    keys = kv.T[0:64].astype(bf16)
    shift = jnp.concatenate([bias_ref[...].astype(f32), jnp.zeros((256, 120), f32)], axis=1).T[0:8]
    shifts = jnp.concatenate([shift, shift], axis=0).astype(bf16)
    v = kv[:, 64:]
    left = jnp.concatenate([v[0:64], v[128:192]], axis=1)
    right = jnp.concatenate([v[64:128], v[192:256]], axis=1)
    out_ref[0:64, :] = keys
    out_ref[64:80, :] = shifts
    out_ref[80:144, :] = jnp.concatenate([left, right], axis=1).astype(bf16)


def pack(key_value, bias):
    return pl.pallas_call(
        pack_kernel,
        out_shape=jax.ShapeDtypeStruct((144, 256), jnp.bfloat16),
        in_specs=[VM, VM],
        out_specs=VM,
        name="pack",
    )(key_value, bias)


def gather_kernel(mine_ref, q_ref, kv_ref, theirs_ref, send, recv_a, recv_b, recv_s, q_send, q_recv, local):
    z, y, c, x = place()
    sp = (z * 4 + y) * 2 + c

    def at(zz, yy, cc):
        return (zz % 4 * 4 + yy % 4) * 2 + cc

    barrier = pltpu.get_barrier_semaphore()
    for d in (1, 2, 3):
        pl.semaphore_signal(barrier, inc=1, device_id=(at(z + d, y, c), x), device_id_type=MESH)
        pl.semaphore_signal(barrier, inc=1, device_id=(at(z, y + d, c), x), device_id_type=MESH)
    pl.semaphore_signal(barrier, inc=1, device_id=(at(z, y, 1 - c), x), device_id_type=MESH)
    pl.semaphore_signal(barrier, inc=1, device_id=(31 - sp, x), device_id_type=MESH)
    own = pltpu.make_async_copy(mine_ref, kv_ref.at[sp], local)
    own.start()
    pl.semaphore_wait(barrier, 8)
    sends = []

    def push(src, dst, recv, device):
        copy = pltpu.make_async_remote_copy(
            src_ref=src, dst_ref=dst, send_sem=send.at[len(sends)], recv_sem=recv, device_id=(device, x), device_id_type=MESH
        )
        copy.start()
        sends.append(copy)

    def part_a(ref, block=None):
        return ref.at[pl.ds(0, 80), :] if block is None else ref.at[block, pl.ds(0, 80), :]

    def part_b(ref, block=None):
        return ref.at[pl.ds(80, 64), :] if block is None else ref.at[block, pl.ds(80, 64), :]

    for d in (1, 3, 2):
        push(part_a(mine_ref), part_a(kv_ref, sp), recv_a.at[d, 0], at(z + d, y, c))
        push(part_b(mine_ref), part_b(kv_ref, sp), recv_b.at[0, d], at(z, y + d, c))
    for d in (1, 3, 2):
        push(part_a(mine_ref), part_a(kv_ref, sp), recv_a.at[0, d], at(z, y + d, c))
        push(part_b(mine_ref), part_b(kv_ref, sp), recv_b.at[d, 0], at(z + d, y, c))
    push(part_a(mine_ref), part_a(kv_ref, sp), recv_s.at[0, 0, 0], at(z, y, 1 - c))
    push(part_b(mine_ref), part_b(kv_ref, sp), recv_s.at[0, 0, 1], at(z, y, 1 - c))
    theirs = pltpu.make_async_remote_copy(
        src_ref=q_ref.at[pl.ds(0, 128), :], dst_ref=theirs_ref, send_sem=q_send, recv_sem=q_recv, device_id=(31 - sp, x), device_id_type=MESH
    )

    @pl.when(sp >= 16)
    def _():
        theirs.start()

    def landed(dz, dy, which):
        block = at(z - dz, y - dy, c)
        ref = part_a(kv_ref, block) if which == 0 else part_b(kv_ref, block)
        sem = (recv_a if which == 0 else recv_b).at[dz, dy]
        pltpu.make_async_copy(ref, ref, sem).wait()
        return ref

    for d in (1, 3, 2):
        ref = landed(d, 0, 0)
        for e in (1, 3, 2):
            push(ref, ref, recv_a.at[d, e], at(z, y + e, c))
        push(ref, ref, recv_s.at[d, 0, 0], at(z, y, 1 - c))
        ref = landed(0, d, 1)
        for e in (1, 3, 2):
            push(ref, ref, recv_b.at[e, d], at(z + e, y, c))
        push(ref, ref, recv_s.at[0, d, 1], at(z, y, 1 - c))
    for d in (1, 3, 2):
        ref = landed(0, d, 0)
        push(ref, ref, recv_s.at[0, d, 0], at(z, y, 1 - c))
        ref = landed(d, 0, 1)
        push(ref, ref, recv_s.at[d, 0, 1], at(z, y, 1 - c))
    for d in (1, 3, 2):
        for e in (1, 3, 2):
            ref = landed(d, e, 0)
            push(ref, ref, recv_s.at[d, e, 0], at(z, y, 1 - c))
            ref = landed(e, d, 1)
            push(ref, ref, recv_s.at[e, d, 1], at(z, y, 1 - c))
    for dz in range(4):
        for dy in range(4):
            block = at(z - dz, y - dy, 1 - c)
            for which in (0, 1):
                ref = part_a(kv_ref, block) if which == 0 else part_b(kv_ref, block)
                pltpu.make_async_copy(ref, ref, recv_s.at[dz, dy, which]).wait()
    own.wait()
    for copy in sends:
        copy.wait_send()

    @pl.when(sp >= 16)
    def _():
        theirs.wait_send()

    @pl.when(sp < 16)
    def _():
        theirs.wait_recv()


def gather(mine, queries):
    return pl.pallas_call(
        gather_kernel,
        out_shape=(jax.ShapeDtypeStruct((32, 144, 256), jnp.bfloat16), jax.ShapeDtypeStruct((128, 512), jnp.bfloat16)),
        in_specs=[VM, VM],
        out_specs=(VM, VM),
        scratch_shapes=[
            pltpu.SemaphoreType.DMA((64,)),
            pltpu.SemaphoreType.DMA((4, 4)),
            pltpu.SemaphoreType.DMA((4, 4)),
            pltpu.SemaphoreType.DMA((4, 4, 2)),
            pltpu.SemaphoreType.DMA,
            pltpu.SemaphoreType.DMA,
            pltpu.SemaphoreType.DMA,
        ],
        compiler_params=pltpu.CompilerParams(collective_id=0, has_side_effects=True),
        name="gather",
    )(mine, queries)


def swap_kernel(thresholds, att_ref, out_ref, send, recv):
    z, y, c, x = place()
    sp = (z * 4 + y) * 2 + c
    other = 31 - sp
    n = given_tiles(sp, thresholds)
    low = sp < 16
    barrier = pltpu.get_barrier_semaphore()
    for d in (1, 2, 3):
        pl.semaphore_signal(barrier, inc=1, device_id=(sp, (x + d) % 4), device_id_type=MESH)
    for d in range(4):
        pl.semaphore_signal(barrier, inc=1, device_id=(other, (x + d) % 4), device_id_type=MESH)
    pl.semaphore_wait(barrier, 7)

    def tile(s):
        return att_ref.at[pl.ds(s * 32, 32), :]

    def spot(t, half):
        return out_ref.at[t, pl.ds(half * 32, 32), :]

    jobs = []
    for d in (1, 3, 2, 0):
        for half in (0, 1):
            s = (x + d) % 4 * 2 + half
            made = jnp.logical_or(low, s >= n)
            if d == 0:
                copy = pltpu.make_async_copy(tile(s), spot(x, half), recv.at[x * 2 + half])
            else:
                copy = pltpu.make_async_remote_copy(
                    src_ref=tile(s), dst_ref=spot(x, half), send_sem=send.at[d * 2 + half], recv_sem=recv.at[x * 2 + half],
                    device_id=(sp, (x + d) % 4), device_id_type=MESH,
                )
            jobs.append((made, copy, d != 0))
    for s in range(len(thresholds)):
        made = jnp.logical_and(low, s < n)
        copy = pltpu.make_async_remote_copy(
            src_ref=tile(8 + s), dst_ref=spot(x, s % 2), send_sem=send.at[8 + s], recv_sem=recv.at[x * 2 + s % 2],
            device_id=(other, s // 2), device_id_type=MESH,
        )
        jobs.append((made, copy, True))
    for made, copy, _ in jobs:
        pl.when(made)(copy.start)
    for t in range(4):
        for half in (0, 1):
            pltpu.make_async_copy(spot(t, half), spot(t, half), recv.at[t * 2 + half]).wait()
    for made, copy, remote in jobs:
        if remote:
            pl.when(made)(copy.wait_send)


def swap(att, thresholds):
    return pl.pallas_call(
        functools.partial(swap_kernel, thresholds),
        out_shape=jax.ShapeDtypeStruct((4, 64, 512), jnp.bfloat16),
        in_specs=[VM],
        out_specs=VM,
        scratch_shapes=[pltpu.SemaphoreType.DMA((12,)), pltpu.SemaphoreType.DMA((8,))],
        compiler_params=pltpu.CompilerParams(collective_id=1, has_side_effects=True),
        name="swap",
    )(att)


def offsets():
    every = [(dz, dy, dx, dc) for dz in range(4) for dy in range(4) for dx in range(4) for dc in range(2)][1:]
    order = np.random.default_rng(1).permutation(len(every))
    return [every[k] for k in order]


def exchange_kernel(x_ref, o_ref, send, recv, local):
    z, y, c, x = place()
    me = ((z * 4 + y) * 2 + c) * 4 + x

    def peer(o):
        return (((z + o[0]) % 4 * 4 + (y + o[1]) % 4) * 2 + (c + o[3]) % 2, (x + o[2]) % 4)

    steps = offsets()
    barrier = pltpu.get_barrier_semaphore()
    for o in steps:
        pl.semaphore_signal(barrier, inc=1, device_id=peer(o), device_id_type=MESH)
    own = pltpu.make_async_copy(x_ref.at[me], o_ref.at[me], local)
    own.start()
    pl.semaphore_wait(barrier, len(steps))
    for o in steps:
        s, t = peer(o)
        pltpu.make_async_remote_copy(
            src_ref=x_ref.at[s * 4 + t], dst_ref=o_ref.at[me], send_sem=send, recv_sem=recv, device_id=(s, t), device_id_type=MESH
        ).start()
    own.wait()
    count = len(steps)
    pltpu.make_async_copy(x_ref.at[pl.ds(0, count)], o_ref.at[pl.ds(0, count)], send).wait()
    pltpu.make_async_copy(x_ref.at[pl.ds(0, count)], o_ref.at[pl.ds(0, count)], recv).wait()


def exchange(x, number):
    return pl.pallas_call(
        exchange_kernel,
        out_shape=jax.ShapeDtypeStruct(x.shape, x.dtype),
        in_specs=[VM],
        out_specs=VM,
        scratch_shapes=[pltpu.SemaphoreType.DMA] * 3,
        compiler_params=pltpu.CompilerParams(collective_id=number, has_side_effects=True, vmem_limit_bytes=32 * 1024 * 1024),
        name="exchange",
    )(x)


def slot_codes(shape, dim):
    at = lax.broadcasted_iota(jnp.int32, shape, dim)
    return at // 8, at // 4 % 2, at % 4


def project_kernel(th_ref, w_ref, stream_ref, gain_ref, routes_ref, sg_ref, su_ref, sd_ref, out_ref, base_ref):
    f32, bf16 = jnp.float32, jnp.bfloat16
    dot = functools.partial(jnp.dot, preferred_element_type=f32)
    mixed = sum(dot(th_ref[t], w_ref[pl.ds(512 * t, 512), :]) for t in range(4))
    resid = (stream_ref[...].astype(f32) + mixed).astype(bf16).astype(f32)
    factor = lax.rsqrt(jnp.mean(resid * resid, axis=1, keepdims=True) + 1e-06)
    normed = (resid * factor * gain_ref[...]).astype(bf16)
    expert = lax.broadcasted_iota(jnp.int32, (128, 64), 0)
    named = jnp.zeros((128, 64), f32)
    for k in range(4):
        named = jnp.where(routes_ref[pl.ds(k, 1), :] == expert, 1.0, named)
    earlier = lax.broadcasted_iota(jnp.int32, (64, 64), 0) < lax.broadcasted_iota(jnp.int32, (64, 64), 1)
    rank = dot(named.astype(bf16), earlier.astype(f32).astype(bf16))
    e, h, k = slot_codes((1024, 128), 0)
    spread = (e == lax.broadcasted_iota(jnp.int32, (1024, 128), 1)).astype(f32).astype(bf16)
    both = dot(spread, jnp.concatenate([named, rank], axis=1).astype(bf16))
    _, h, k = slot_codes((1024, 64), 0)
    taken = jnp.where(both[:, 64:] == k.astype(f32), both[:, :64], 0.0)
    pick = jnp.concatenate([jnp.where(h == 0, taken, 0.0), jnp.where(h == 1, taken, 0.0)], axis=1).astype(bf16)
    out_ref[...] = dot(pick, jnp.concatenate([normed[:, :1024], normed[:, 1024:]], axis=0)).astype(bf16)
    gate = dot(normed, sg_ref[...])
    inner = (gate * jax.nn.sigmoid(gate) * dot(normed, su_ref[...])).astype(bf16)
    base_ref[...] = resid + dot(inner, sd_ref[...])


def project(th, w, stream, gain, routes_t, sg, su, sd):
    return pl.pallas_call(
        project_kernel,
        out_shape=(jax.ShapeDtypeStruct((1024, 1024), jnp.bfloat16), jax.ShapeDtypeStruct((64, 2048), jnp.float32)),
        in_specs=[VM] * 8,
        out_specs=(VM, VM),
        compiler_params=pltpu.CompilerParams(vmem_limit_bytes=48 * 1024 * 1024),
        name="project",
    )(th, w, stream, gain, routes_t, sg, su, sd)


def expert_kernel(x_ref, g_ref, u_ref, d_ref, out_ref):
    f32, bf16 = jnp.float32, jnp.bfloat16
    dot = functools.partial(jnp.dot, preferred_element_type=f32)
    top = lax.broadcasted_iota(jnp.int32, (16, 8, 1024), 1) < 4

    def some(j, _):
        rows = pl.ds(j * 256, 256)
        wide = x_ref[rows, :].astype(f32).reshape(16, 2, 8, 1024)
        a, b = wide[:, 0], wide[:, 1]
        left = jnp.where(top, a, pltpu.roll(b, 4, 1)).reshape(128, 1024).astype(bf16)
        right = jnp.where(top, pltpu.roll(a, 4, 1), b).reshape(128, 1024).astype(bf16)
        gate = dot(left, g_ref[0:1024, :]) + dot(right, g_ref[1024:2048, :])
        up = dot(left, u_ref[0:1024, :]) + dot(right, u_ref[1024:2048, :])
        inner = (gate * jax.nn.sigmoid(gate) * up).astype(bf16)
        lo = dot(inner, d_ref[:, 0:1024]).reshape(16, 8, 1024)
        hi = dot(inner, d_ref[:, 1024:2048]).reshape(16, 8, 1024)
        first = jnp.where(top, lo, pltpu.roll(hi, 4, 1))
        second = jnp.where(top, pltpu.roll(lo, 4, 1), hi)
        out_ref[rows, :] = jnp.stack([first, second], axis=1).reshape(256, 1024).astype(bf16)
        return 0

    lax.fori_loop(0, 4, some, 0)


def experts(x, g, u, d):
    return pl.pallas_call(
        expert_kernel,
        out_shape=jax.ShapeDtypeStruct((1024, 1024), jnp.bfloat16),
        in_specs=[VM] * 4,
        out_specs=VM,
        compiler_params=pltpu.CompilerParams(vmem_limit_bytes=48 * 1024 * 1024),
        name="experts",
    )(x, g, u, d)


def combine_kernel(back_ref, base_ref, routes_ref, score_ref, out_ref):
    f32, bf16 = jnp.float32, jnp.bfloat16
    dot = functools.partial(jnp.dot, preferred_element_type=f32)
    score = score_ref[...]
    gates = 2.5 * score / jnp.sum(score, axis=1, keepdims=True)
    expert = lax.broadcasted_iota(jnp.int32, (64, 128), 1)
    named = jnp.zeros((64, 128), f32)
    gate = jnp.zeros((64, 128), f32)
    for k in range(4):
        hit = routes_ref[:, k : k + 1] == expert
        named = jnp.where(hit, 1.0, named)
        gate = jnp.where(hit, gates[:, k : k + 1], gate)
    earlier = lax.broadcasted_iota(jnp.int32, (64, 64), 1) < lax.broadcasted_iota(jnp.int32, (64, 64), 0)
    rank = dot(earlier.astype(f32).astype(bf16), named.astype(bf16))
    high = gate.astype(bf16)
    low = (gate - high.astype(f32)).astype(bf16)
    e, _, _ = slot_codes((128, 1024), 1)
    spread = (e == lax.broadcasted_iota(jnp.int32, (128, 1024), 0)).astype(f32).astype(bf16)
    wide = dot(jnp.concatenate([rank.astype(bf16), high, low], axis=0), spread)
    _, h, k = slot_codes((64, 1024), 1)
    mine = wide[0:64] == k.astype(f32)
    parts = []
    for half in (0, 1):
        for piece in (wide[64:128], wide[128:192]):
            parts.append(jnp.where(mine & (h == half), piece, 0.0))
    total = dot(jnp.concatenate(parts, axis=0).astype(bf16), back_ref[...])
    base = base_ref[...]
    out_ref[:, 0:1024] = (base[:, 0:1024] + total[0:64] + total[64:128]).astype(bf16)
    out_ref[:, 1024:2048] = (base[:, 1024:2048] + total[128:192] + total[192:256]).astype(bf16)


def combine(back, base, routes, score):
    return pl.pallas_call(
        combine_kernel,
        out_shape=jax.ShapeDtypeStruct((64, 2048), jnp.bfloat16),
        in_specs=[VM] * 4,
        out_specs=VM,
        compiler_params=pltpu.CompilerParams(vmem_limit_bytes=32 * 1024 * 1024),
        name="combine",
    )(back, base, routes, score)


def body(
    queries, key_value, break_bias, stream, out_proj, ffn_gain, routes, route_score,
    expert_gate, expert_up, expert_down, shared_gate, shared_up, shared_down,
):
    table, give, diag_groups, _ = schedule(lax.axis_size("sp"), queries.shape[0] // 32, GROUP)
    thresholds = tuple(int((give >= k).sum()) for k in range(1, int(give.max()) + 1))
    kv, theirs = gather(pack(key_value[:, 0, :], break_bias), queries)
    tab = lax.dynamic_index_in_dim(jnp.asarray(table), lax.axis_index("sp"), 0, keepdims=False)
    made = attend(tab, jnp.concatenate([queries, theirs], axis=0), kv, GROUP, diag_groups)
    heads = swap(made, thresholds)
    outgoing, base = project(
        heads, out_proj, stream, ffn_gain.reshape(1, -1), routes.T, shared_gate, shared_up, shared_down
    )
    arrived = exchange(outgoing.reshape(128, 8, 1024), 2)
    done = experts(arrived.reshape(1024, 1024), expert_gate[0], expert_up[0], expert_down[0])
    back = exchange(done.reshape(128, 8, 1024), 3)
    return combine(back.reshape(1024, 1024), base, routes, route_score)


def solution(mesh):
    return jax.shard_map(
        body,
        mesh=mesh,
        in_specs=(
            P("sp", "tp"),
            P("sp", "tp", None),
            P("sp", "tp"),
            P(("sp", "tp"), None),
            P(),
            P(),
            P(("sp", "tp"), None),
            P(("sp", "tp"), None),
            P(("sp", "tp"), None, None),
            P(("sp", "tp"), None, None),
            P(("sp", "tp"), None, None),
            P(),
            P(),
            P(),
        ),
        out_specs=P(("sp", "tp"), None),
        check_vma=False,
    )
```

```python
import functools

import jax
import jax.numpy as jnp
import numpy as np
from jax import lax
from jax.experimental import pallas as pl
from jax.experimental.pallas import tpu as pltpu
from jax.sharding import PartitionSpec as P

GROUP = 8
LOG2E = 1.4426950408889634


def schedule(blocks, tiles, group):
    half = blocks // 2
    rows = []
    give = []
    for i in range(half):
        best = min(range(0, tiles // 2 + 1), key=lambda n: max(tiles * (i + 1) + n * (blocks - i), (tiles - n) * (blocks - i)))
        give.append(best)
    for i in range(blocks):
        n = give[min(i, blocks - 1 - i)]
        if i < half:
            slots = [(s, i) for s in range(tiles)] + [(tiles + s, blocks - 1 - i) for s in range(n)]
        else:
            slots = [(s, i) for s in range(n, tiles)]
        diag = [(s, q) for s, q in slots]
        main = []
        depth = max(q for _, q in slots)
        for back in range(1, depth + 1):
            for s, q in slots:
                if q - back >= 0:
                    main.append((s, q - back))
        rows.append((diag, main))
    spare = tiles + tiles // 2
    ld = max(-(-len(d) // group) for d, _ in rows)
    lm = max(-(-len(m) // group) for _, m in rows)
    table = np.zeros((blocks, 2 + 2 * group * (ld + lm)), np.int32)
    for i, (diag, main) in enumerate(rows):
        nd, nm = -(-len(diag) // group), -(-len(main) // group)
        diag = diag + [(spare, 0)] * (group * ld - len(diag))
        main = main + [(spare, 0)] * (group * lm - len(main))
        table[i, 0], table[i, 1] = nd, nm
        table[i, 2:] = np.array(diag + main).reshape(-1)
    return table, np.array(give), ld, lm


def attend_kernel(group, ld, tab, q_ref, kv_ref, tri_ref, out_ref, qs, acc, carry):
    nt = out_ref.shape[0] // 32
    f32, bf16 = jnp.float32, jnp.bfloat16
    head_lane = lax.broadcasted_iota(jnp.int32, (32, 16), 1)
    c_hi = float(np.asarray(LOG2E, jnp.bfloat16))
    c_lo = float(np.float32(LOG2E - c_hi))

    def build(s, _):
        q = q_ref[pl.ds(s * 32, 32), :].astype(f32) * (0.125 * LOG2E)
        hi = q.astype(bf16)
        lo = (q - hi.astype(f32)).astype(bf16)
        for h in range(8):
            tail = jnp.where(head_lane == h, c_hi, jnp.where(head_lane == h + 8, c_lo, 0.0)).astype(bf16)
            qs[s, pl.ds(h * 32, 32), :] = jnp.concatenate([hi[:, 64 * h:64 * h + 64], lo[:, 64 * h:64 * h + 64], tail], axis=1)
        return 0

    lax.fori_loop(0, nt, build, 0)
    qs[nt] = jnp.zeros_like(qs[nt])
    acc[...] = jnp.zeros_like(acc)
    carry[...] = jnp.zeros_like(carry)
    lane = lax.broadcasted_iota(jnp.int32, (128, 128), 1)

    def step(base, masked):
        for g in range(group):
            slot = tab[base + 2 * g]
            chunk = tab[base + 2 * g + 1]
            key = jnp.concatenate([kv_ref[chunk, 0:64, :], kv_ref[chunk, 0:80, :]], axis=0)
            z = jnp.dot(qs[slot], key, preferred_element_type=f32)
            if masked:
                row = lax.broadcasted_iota(jnp.int32, (256, 256), 0) % 32 + (slot % 8) * 32
                col = lax.broadcasted_iota(jnp.int32, (256, 256), 1)
                z = jnp.where(col < row, z, -1e30)
            sp = jnp.maximum(z, lax.log2(1.0 + jnp.exp2(jnp.minimum(z, 126.0))))
            u = z - sp
            sums = jnp.dot(sp.astype(bf16), tri_ref[...], preferred_element_type=f32)
            before = carry[slot]
            w = jnp.exp2(u - sums[:, :256] - jnp.concatenate([before, before], axis=1)).astype(bf16)
            carry[slot] = before + sums[:, 256:]
            vx = kv_ref[chunk, 80:144, :]
            v = jnp.concatenate([vx[:, :128], vx[:, 128:]], axis=0)
            zero = jnp.zeros_like(v)
            both = jnp.concatenate([jnp.where(lane < 64, v, zero), jnp.where(lane < 64, zero, v)], axis=0)
            acc[slot] += jnp.dot(w, both, preferred_element_type=f32)

    def diag_step(j, _):
        step(2 + 2 * group * j, True)
        return 0

    def main_step(j, _):
        step(2 + 2 * group * (ld + j), False)
        return 0

    lax.fori_loop(0, tab[0], diag_step, 0)
    lax.fori_loop(0, tab[1], main_step, 0)

    def finish(s, _):
        for p in range(4):
            pair = []
            for h in (2 * p, 2 * p + 1):
                a = acc[s, pl.ds(h * 32, 32), :]
                pair.append(a[:, :64] + a[:, 64:])
            out_ref[pl.ds(s * 32, 32), pl.ds(128 * p, 128)] = jnp.concatenate(pair, axis=1).astype(bf16)
        return 0

    lax.fori_loop(0, nt, finish, 0)


def triangle():
    t = np.zeros((256, 384), np.float32)
    t[:, :256] = np.tril(np.ones((256, 256)), -1)
    t[:, 256:] = 1.0
    return t


def attend(tab, q_all, kv, group, ld):
    nt = q_all.shape[0] // 32
    vm = pl.BlockSpec(memory_space=pltpu.VMEM)
    return pl.pallas_call(
        functools.partial(attend_kernel, group, ld),
        out_shape=jax.ShapeDtypeStruct(q_all.shape, jnp.bfloat16),
        in_specs=[pl.BlockSpec(memory_space=pltpu.SMEM), vm, vm, vm],
        out_specs=vm,
        scratch_shapes=[pltpu.VMEM((nt + 1, 256, 144), jnp.bfloat16), pltpu.VMEM((nt + 1, 256, 128), jnp.float32), pltpu.VMEM((nt + 1, 256, 128), jnp.float32)],
        compiler_params=pltpu.CompilerParams(vmem_limit_bytes=48 * 1024 * 1024),
        name="attend",
    )(tab, q_all, kv, jnp.asarray(triangle(), jnp.bfloat16))


MESH = pl.DeviceIdType.MESH
VM = pl.BlockSpec(memory_space=pltpu.VMEM)


def place():
    sp, x = lax.axis_index("sp"), lax.axis_index("tp")
    return sp // 8, (sp // 2) % 4, sp % 2, x


def given_tiles(sp, thresholds):
    low = jnp.minimum(sp, 31 - sp)
    n = jnp.int32(0)
    for t in thresholds:
        n = n + jnp.where(low < t, 1, 0)
    return n


def pack_kernel(kv_ref, bias_ref, out_ref):
    f32, bf16 = jnp.float32, jnp.bfloat16
    kv = kv_ref[...].astype(f32)
    keys = kv.T[0:64].astype(bf16)
    shift = jnp.concatenate([bias_ref[...].astype(f32), jnp.zeros((256, 120), f32)], axis=1).T[0:8]
    shifts = jnp.concatenate([shift, shift], axis=0).astype(bf16)
    v = kv[:, 64:]
    left = jnp.concatenate([v[0:64], v[128:192]], axis=1)
    right = jnp.concatenate([v[64:128], v[192:256]], axis=1)
    out_ref[0:64, :] = keys
    out_ref[64:80, :] = shifts
    out_ref[80:144, :] = jnp.concatenate([left, right], axis=1).astype(bf16)


def pack(key_value, bias):
    return pl.pallas_call(
        pack_kernel,
        out_shape=jax.ShapeDtypeStruct((144, 256), jnp.bfloat16),
        in_specs=[VM, VM],
        out_specs=VM,
        name="pack",
    )(key_value, bias)


def gather_kernel(mine_ref, q_ref, kv_ref, theirs_ref, send, recv_a, recv_b, recv_s, q_send, q_recv, local):
    z, y, c, x = place()
    sp = (z * 4 + y) * 2 + c

    def at(zz, yy, cc):
        return (zz % 4 * 4 + yy % 4) * 2 + cc

    barrier = pltpu.get_barrier_semaphore()
    for d in (1, 2, 3):
        pl.semaphore_signal(barrier, inc=1, device_id=(at(z + d, y, c), x), device_id_type=MESH)
        pl.semaphore_signal(barrier, inc=1, device_id=(at(z, y + d, c), x), device_id_type=MESH)
    pl.semaphore_signal(barrier, inc=1, device_id=(at(z, y, 1 - c), x), device_id_type=MESH)
    pl.semaphore_signal(barrier, inc=1, device_id=(31 - sp, x), device_id_type=MESH)
    own = pltpu.make_async_copy(mine_ref, kv_ref.at[sp], local)
    own.start()
    pl.semaphore_wait(barrier, 8)
    sends = []

    def push(src, dst, recv, device):
        copy = pltpu.make_async_remote_copy(
            src_ref=src, dst_ref=dst, send_sem=send.at[len(sends)], recv_sem=recv, device_id=(device, x), device_id_type=MESH
        )
        copy.start()
        sends.append(copy)

    def part_a(ref, block=None):
        return ref.at[pl.ds(0, 80), :] if block is None else ref.at[block, pl.ds(0, 80), :]

    def part_b(ref, block=None):
        return ref.at[pl.ds(80, 64), :] if block is None else ref.at[block, pl.ds(80, 64), :]

    for d in (1, 3, 2):
        push(part_a(mine_ref), part_a(kv_ref, sp), recv_a.at[d, 0], at(z + d, y, c))
        push(part_b(mine_ref), part_b(kv_ref, sp), recv_b.at[0, d], at(z, y + d, c))
    for d in (1, 3, 2):
        push(part_a(mine_ref), part_a(kv_ref, sp), recv_a.at[0, d], at(z, y + d, c))
        push(part_b(mine_ref), part_b(kv_ref, sp), recv_b.at[d, 0], at(z + d, y, c))
    push(part_a(mine_ref), part_a(kv_ref, sp), recv_s.at[0, 0, 0], at(z, y, 1 - c))
    push(part_b(mine_ref), part_b(kv_ref, sp), recv_s.at[0, 0, 1], at(z, y, 1 - c))
    theirs = pltpu.make_async_remote_copy(
        src_ref=q_ref.at[pl.ds(0, 128), :], dst_ref=theirs_ref, send_sem=q_send, recv_sem=q_recv, device_id=(31 - sp, x), device_id_type=MESH
    )

    @pl.when(sp >= 16)
    def _():
        theirs.start()

    def landed(dz, dy, which):
        block = at(z - dz, y - dy, c)
        ref = part_a(kv_ref, block) if which == 0 else part_b(kv_ref, block)
        sem = (recv_a if which == 0 else recv_b).at[dz, dy]
        pltpu.make_async_copy(ref, ref, sem).wait()
        return ref

    for d in (1, 3, 2):
        ref = landed(d, 0, 0)
        for e in (1, 3, 2):
            push(ref, ref, recv_a.at[d, e], at(z, y + e, c))
        push(ref, ref, recv_s.at[d, 0, 0], at(z, y, 1 - c))
        ref = landed(0, d, 1)
        for e in (1, 3, 2):
            push(ref, ref, recv_b.at[e, d], at(z + e, y, c))
        push(ref, ref, recv_s.at[0, d, 1], at(z, y, 1 - c))
    for d in (1, 3, 2):
        ref = landed(0, d, 0)
        push(ref, ref, recv_s.at[0, d, 0], at(z, y, 1 - c))
        ref = landed(d, 0, 1)
        push(ref, ref, recv_s.at[d, 0, 1], at(z, y, 1 - c))
    for d in (1, 3, 2):
        for e in (1, 3, 2):
            ref = landed(d, e, 0)
            push(ref, ref, recv_s.at[d, e, 0], at(z, y, 1 - c))
            ref = landed(e, d, 1)
            push(ref, ref, recv_s.at[e, d, 1], at(z, y, 1 - c))
    for dz in range(4):
        for dy in range(4):
            block = at(z - dz, y - dy, 1 - c)
            for which in (0, 1):
                ref = part_a(kv_ref, block) if which == 0 else part_b(kv_ref, block)
                pltpu.make_async_copy(ref, ref, recv_s.at[dz, dy, which]).wait()
    own.wait()
    for copy in sends:
        copy.wait_send()

    @pl.when(sp >= 16)
    def _():
        theirs.wait_send()

    @pl.when(sp < 16)
    def _():
        theirs.wait_recv()


def gather(mine, queries):
    return pl.pallas_call(
        gather_kernel,
        out_shape=(jax.ShapeDtypeStruct((32, 144, 256), jnp.bfloat16), jax.ShapeDtypeStruct((128, 512), jnp.bfloat16)),
        in_specs=[VM, VM],
        out_specs=(VM, VM),
        scratch_shapes=[
            pltpu.SemaphoreType.DMA((64,)),
            pltpu.SemaphoreType.DMA((4, 4)),
            pltpu.SemaphoreType.DMA((4, 4)),
            pltpu.SemaphoreType.DMA((4, 4, 2)),
            pltpu.SemaphoreType.DMA,
            pltpu.SemaphoreType.DMA,
            pltpu.SemaphoreType.DMA,
        ],
        compiler_params=pltpu.CompilerParams(collective_id=0, has_side_effects=True),
        name="gather",
    )(mine, queries)


def offsets():
    every = [(dz, dy, dx, dc) for dz in range(4) for dy in range(4) for dx in range(4) for dc in range(2)][1:]
    order = np.random.default_rng(1).permutation(len(every))
    return [every[k] for k in order]


def slot_codes(shape, dim):
    at = lax.broadcasted_iota(jnp.int32, shape, dim)
    return at // 8, at // 4 % 2, at % 4


GROUPS = 4


def layer_kernel(
    thresholds, att_ref, w_hbm, stream_ref, gain_ref, routes_ref, routes_t_ref, score_ref, sg_hbm, su_hbm, sd_hbm, g_hbm, u_hbm, d_hbm,
    out_ref, w_ref, sg_ref, su_ref, sd_ref, g_ref, u_ref, d_ref, heads, leaving, arrived, done, back,
    load, swap_send, swap_recv, go_send, go_recv, back_send, back_recv, own_sem,
):
    f32, bf16 = jnp.float32, jnp.bfloat16
    dot = functools.partial(jnp.dot, preferred_element_type=f32)
    z, y, c, x = place()
    sp = (z * 4 + y) * 2 + c
    me = sp * 4 + x
    other = 31 - sp
    n = given_tiles(sp, thresholds)
    low = sp < 16
    steps = offsets()

    def peer(o, way=1):
        return (((z + way * o[0]) % 4 * 4 + (y + way * o[1]) % 4) * 2 + (c + o[3]) % 2, (x + way * o[2]) % 4)

    barrier = pltpu.get_barrier_semaphore()
    for o in steps:
        pl.semaphore_signal(barrier, inc=1, device_id=peer(o), device_id_type=MESH)
    loads = []
    for k, (src, dst) in enumerate(
        ((w_hbm, w_ref), (sg_hbm, sg_ref), (su_hbm, su_ref), (sd_hbm, sd_ref), (g_hbm, g_ref), (u_hbm, u_ref), (d_hbm, d_ref))
    ):
        loads.append(pltpu.make_async_copy(src, dst, load.at[k]))
        loads[-1].start()
    pl.semaphore_wait(barrier, len(steps))

    def tile(s):
        return att_ref.at[pl.ds(s * 32, 32), :]

    def spot(t, half):
        return heads.at[t, pl.ds(half * 32, 32), :]

    jobs = []
    for d in (1, 3, 2, 0):
        for half in (0, 1):
            s = (x + d) % 4 * 2 + half
            made = jnp.logical_or(low, s >= n)
            if d == 0:
                copy = pltpu.make_async_copy(tile(s), spot(x, half), swap_recv.at[x * 2 + half])
            else:
                copy = pltpu.make_async_remote_copy(
                    src_ref=tile(s), dst_ref=spot(x, half), send_sem=swap_send.at[d * 2 + half], recv_sem=swap_recv.at[x * 2 + half],
                    device_id=(sp, (x + d) % 4), device_id_type=MESH,
                )
            jobs.append((made, copy, d != 0))
    for s in range(len(thresholds)):
        made = jnp.logical_and(low, s < n)
        copy = pltpu.make_async_remote_copy(
            src_ref=tile(8 + s), dst_ref=spot(x, s % 2), send_sem=swap_send.at[8 + s], recv_sem=swap_recv.at[x * 2 + s % 2],
            device_id=(other, s // 2), device_id_type=MESH,
        )
        jobs.append((made, copy, True))
    for made, copy, _ in jobs:
        pl.when(made)(copy.start)

    expert = lax.broadcasted_iota(jnp.int32, (128, 64), 0)
    named = jnp.zeros((128, 64), f32)
    for k in range(4):
        named = jnp.where(routes_t_ref[pl.ds(k, 1), :] == expert, 1.0, named)
    earlier = lax.broadcasted_iota(jnp.int32, (64, 64), 0) < lax.broadcasted_iota(jnp.int32, (64, 64), 1)
    rank = dot(named.astype(bf16), earlier.astype(f32).astype(bf16))
    e, _, _ = slot_codes((1024, 128), 0)
    spread = (e == lax.broadcasted_iota(jnp.int32, (1024, 128), 1)).astype(f32).astype(bf16)
    both = dot(spread, jnp.concatenate([named, rank], axis=1).astype(bf16))
    _, h, k = slot_codes((1024, 64), 0)
    taken = jnp.where(both[:, 64:] == k.astype(f32), both[:, :64], 0.0)
    pick = jnp.concatenate([jnp.where(h == 0, taken, 0.0), jnp.where(h == 1, taken, 0.0)], axis=1).astype(bf16)

    loads[0].wait()
    for t in range(4):
        for half in (0, 1):
            pltpu.make_async_copy(spot(t, half), spot(t, half), swap_recv.at[t * 2 + half]).wait()
    mixed = sum(dot(heads[t], w_ref[pl.ds(512 * t, 512), :]) for t in range(4))
    resid = (stream_ref[...].astype(f32) + mixed).astype(bf16).astype(f32)
    factor = lax.rsqrt(jnp.mean(resid * resid, axis=1, keepdims=True) + 1e-06)
    normed = (resid * factor * gain_ref[...]).astype(bf16)
    picked = dot(pick, jnp.concatenate([normed[:, :1024], normed[:, 1024:]], axis=0))
    leaving[...] = picked.reshape(128, 8, 1024).astype(bf16)

    size = 128 // GROUPS
    places = list(range(len(steps) + 1))
    for j, o in enumerate(steps):
        s, t = peer(o)
        pltpu.make_async_remote_copy(
            src_ref=leaving.at[s * 4 + t], dst_ref=arrived.at[j], send_sem=go_send, recv_sem=go_recv.at[j // size],
            device_id=(s, t), device_id_type=MESH,
        ).start()
    pltpu.make_async_copy(leaving.at[me], arrived.at[127], go_recv.at[GROUPS - 1]).start()

    for k in (1, 2, 3):
        loads[k].wait()
    gate = dot(normed, sg_ref[...])
    inner = (gate * jax.nn.sigmoid(gate) * dot(normed, su_ref[...])).astype(bf16)
    base = resid + dot(inner, sd_ref[...])
    score = score_ref[...]
    gates = 2.5 * score / jnp.sum(score, axis=1, keepdims=True)
    expert = lax.broadcasted_iota(jnp.int32, (64, 128), 1)
    named = jnp.zeros((64, 128), f32)
    gate = jnp.zeros((64, 128), f32)
    for k in range(4):
        hit = routes_ref[:, k : k + 1] == expert
        named = jnp.where(hit, 1.0, named)
        gate = jnp.where(hit, gates[:, k : k + 1], gate)
    earlier = lax.broadcasted_iota(jnp.int32, (64, 64), 1) < lax.broadcasted_iota(jnp.int32, (64, 64), 0)
    rank = dot(earlier.astype(f32).astype(bf16), named.astype(bf16))
    high = gate.astype(bf16)
    small = (gate - high.astype(f32)).astype(bf16)
    e, _, _ = slot_codes((128, 1024), 1)
    spread = (e == lax.broadcasted_iota(jnp.int32, (128, 1024), 0)).astype(f32).astype(bf16)
    wide = dot(jnp.concatenate([rank.astype(bf16), high, small], axis=0), spread)
    _, h, k = slot_codes((64, 1024), 1)
    mine = wide[0:64] == k.astype(f32)
    parts = []
    for half in (0, 1):
        for piece in (wide[64:128], wide[128:192]):
            parts.append(jnp.where(mine & (h == half), piece, 0.0))
    weigh = jnp.concatenate(parts, axis=0).astype(bf16)

    for k in (4, 5, 6):
        loads[k].wait()
    top = lax.broadcasted_iota(jnp.int32, (size // 2, 8, 1024), 1) < 4
    for q in range(GROUPS):
        rows = pl.ds(q * size, size)
        pltpu.make_async_copy(arrived.at[rows], arrived.at[rows], go_recv.at[q]).wait()
        wide = arrived[rows].astype(f32).reshape(size // 2, 2, 8, 1024)
        a, b = wide[:, 0], wide[:, 1]
        left = jnp.where(top, a, pltpu.roll(b, 4, 1)).reshape(size * 4, 1024).astype(bf16)
        right = jnp.where(top, pltpu.roll(a, 4, 1), b).reshape(size * 4, 1024).astype(bf16)
        gate = dot(left, g_ref[0:1024, :]) + dot(right, g_ref[1024:2048, :])
        up = dot(left, u_ref[0:1024, :]) + dot(right, u_ref[1024:2048, :])
        inner = (gate * jax.nn.sigmoid(gate) * up).astype(bf16)
        lo = dot(inner, d_ref[:, 0:1024]).reshape(size // 2, 8, 1024)
        hi = dot(inner, d_ref[:, 1024:2048]).reshape(size // 2, 8, 1024)
        first = jnp.where(top, lo, pltpu.roll(hi, 4, 1))
        second = jnp.where(top, pltpu.roll(lo, 4, 1), hi)
        done[rows] = jnp.stack([first, second], axis=1).reshape(size, 8, 1024).astype(bf16)
        for j in range(q * size, (q + 1) * size):
            if j < len(steps):
                s, t = peer(steps[j], -1)
                pltpu.make_async_remote_copy(
                    src_ref=done.at[j], dst_ref=back.at[me], send_sem=back_send, recv_sem=back_recv,
                    device_id=(s, t), device_id_type=MESH,
                ).start()
            else:
                pltpu.make_async_copy(done.at[j], back.at[me], back_recv).start()

    pltpu.make_async_copy(back, back, back_recv).wait()
    total = dot(weigh, back[...].reshape(1024, 1024))
    out_ref[:, 0:1024] = (base[:, 0:1024] + total[0:64] + total[64:128]).astype(bf16)
    out_ref[:, 1024:2048] = (base[:, 1024:2048] + total[128:192] + total[192:256]).astype(bf16)
    for made, copy, remote in jobs:
        if remote:
            pl.when(made)(copy.wait_send)
    count = pl.ds(0, len(steps))
    pltpu.make_async_copy(leaving.at[count], arrived.at[count], go_send).wait()
    pltpu.make_async_copy(done.at[count], back.at[count], back_send).wait()


def layer(att, thresholds, w, stream, gain, routes, score, sg, su, sd, g, u, d):
    bf16 = jnp.bfloat16
    hbm = pl.BlockSpec(memory_space=pl.ANY)
    chunk = pltpu.VMEM((128, 8, 1024), bf16)
    dma = pltpu.SemaphoreType.DMA
    return pl.pallas_call(
        functools.partial(layer_kernel, thresholds),
        out_shape=jax.ShapeDtypeStruct(stream.shape, bf16),
        in_specs=[VM, hbm, VM, VM, VM, VM, VM, hbm, hbm, hbm, hbm, hbm, hbm],
        out_specs=VM,
        scratch_shapes=[pltpu.VMEM(a.shape, bf16) for a in (w, sg, su, sd, g, u, d)]
        + [pltpu.VMEM((4, 64, 512), bf16), chunk, chunk, chunk, chunk]
        + [dma((7,)), dma((12,)), dma((8,)), dma, dma((GROUPS,)), dma, dma, dma],
        compiler_params=pltpu.CompilerParams(collective_id=1, has_side_effects=True, vmem_limit_bytes=56 * 1024 * 1024),
        name="layer",
    )(att, w, stream, gain, routes, routes.T, score, sg, su, sd, g, u, d)


def body(
    queries, key_value, break_bias, stream, out_proj, ffn_gain, routes, route_score,
    expert_gate, expert_up, expert_down, shared_gate, shared_up, shared_down,
):
    table, give, diag_groups, _ = schedule(lax.axis_size("sp"), queries.shape[0] // 32, GROUP)
    thresholds = tuple(int((give >= k).sum()) for k in range(1, int(give.max()) + 1))
    kv, theirs = gather(pack(key_value[:, 0, :], break_bias), queries)
    tab = lax.dynamic_index_in_dim(jnp.asarray(table), lax.axis_index("sp"), 0, keepdims=False)
    made = attend(tab, jnp.concatenate([queries, theirs], axis=0), kv, GROUP, diag_groups)
    return layer(
        made, thresholds, out_proj, stream, ffn_gain.reshape(1, -1), routes, route_score,
        shared_gate, shared_up, shared_down, expert_gate[0], expert_up[0], expert_down[0],
    )


def solution(mesh):
    return jax.shard_map(
        body,
        mesh=mesh,
        in_specs=(
            P("sp", "tp"),
            P("sp", "tp", None),
            P("sp", "tp"),
            P(("sp", "tp"), None),
            P(),
            P(),
            P(("sp", "tp"), None),
            P(("sp", "tp"), None),
            P(("sp", "tp"), None, None),
            P(("sp", "tp"), None, None),
            P(("sp", "tp"), None, None),
            P(),
            P(),
            P(),
        ),
        out_specs=P(("sp", "tp"), None),
        check_vma=False,
    )
```

```python
import functools

import jax
import jax.numpy as jnp
import numpy as np
from jax import lax
from jax.experimental import pallas as pl
from jax.experimental.pallas import tpu as pltpu
from jax.sharding import PartitionSpec as P

GROUP = 4
LOG2E = 1.4426950408889634


def schedule(blocks, tiles, group):
    half = blocks // 2
    give = []
    for i in range(half):
        give.append(min(range(tiles // 2 + 1), key=lambda n: max(tiles * (i + 1) + n * (blocks - i), (tiles - n) * (blocks - i))))
    spare = tiles + tiles // 2
    lists = []
    for i in range(blocks):
        n = give[min(i, blocks - 1 - i)]
        if i < half:
            slots = [(s, i) for s in range(tiles)] + [(tiles + s, blocks - 1 - i) for s in range(n)]
        else:
            slots = [(s, i) for s in range(n, tiles)]
        left = {s: q + 1 for s, q in slots}
        own = dict(slots)
        groups = []
        while any(left.values()):
            chosen = sorted((s for s in left if left[s]), key=lambda s: -left[s])[:group]
            cells = []
            for s in chosen:
                back = own[s] + 1 - left[s]
                cells.append((s, own[s] - back, 256 * back + 32 * (s % tiles)))
                left[s] -= 1
            groups.append(cells + [(spare, 0, 0)] * (group - len(cells)))
        lists.append(groups)
    longest = max(len(g) for g in lists)
    table = np.zeros((blocks, 1 + 3 * group * (longest + 3)), np.int32)
    for i, groups in enumerate(lists):
        table[i, 0] = -(-len(groups) // 2)
        flat = groups + [[(spare, 0, 0)] * group] * (longest + 3 - len(groups))
        table[i, 1:] = np.array(flat).reshape(-1)
    return table, np.array(give)


def attend_kernel(group, tab, q_ref, more_ref, kv_ref, tri_ref, out_ref, qs, acc, carry, gap, ub, sb):
    nt = out_ref.shape[0] // 32
    sp = lax.axis_index("sp")
    f32, bf16 = jnp.float32, jnp.bfloat16
    head_lane = lax.broadcasted_iota(jnp.int32, (32, 128), 1)
    c_hi = float(np.asarray(LOG2E, jnp.bfloat16))
    c_lo = float(np.float32(LOG2E - c_hi))

    def build(ref, base, s, _):
        q = ref[pl.ds(s * 32, 32), :].astype(f32) * (0.125 * LOG2E)
        s = s + base
        hi = q.astype(bf16)
        lo = (q - hi.astype(f32)).astype(bf16)
        for h in range(8):
            tail = jnp.where(head_lane == h, c_hi, jnp.where(head_lane == h + 8, c_lo, 0.0)).astype(bf16)
            qs[s, pl.ds(h * 32, 32), :] = jnp.concatenate([hi[:, 64 * h:64 * h + 64], lo[:, 64 * h:64 * h + 64], tail], axis=1)
        acc[s] = jnp.zeros((256, 128), f32)
        carry[s] = jnp.zeros((256, 128), f32)
        return 0

    lax.fori_loop(0, nt * 2 // 3, functools.partial(build, q_ref, 0), 0)
    lax.fori_loop(0, nt // 3, functools.partial(build, more_ref, nt * 2 // 3), 0)
    qs[nt] = jnp.zeros_like(qs[nt])
    acc[nt] = jnp.zeros((256, 128), f32)
    carry[nt] = jnp.zeros((256, 128), f32)
    gap[...] = lax.broadcasted_iota(jnp.int32, (256, 256), 1) - lax.broadcasted_iota(jnp.int32, (256, 256), 0) % 32
    lane = lax.broadcasted_iota(jnp.int32, (128, 128), 1)
    blank = jnp.zeros((112, 256), bf16)
    last = lax.broadcasted_iota(jnp.int32, (256, 128), 1) == 127

    def cell(k, g):
        at = 1 + 3 * (group * k + g)
        return tab[sp, at], tab[sp, at + 1], tab[sp, at + 2]

    def first(k, buf):
        for g in range(group):
            slot, chunk, bound = cell(k, g)
            key = jnp.concatenate([kv_ref[chunk, 0:64, :], kv_ref[chunk, 0:80, :], blank], axis=0)
            z = jnp.dot(qs[slot], key, preferred_element_type=f32)
            z = jnp.where(gap[...] < bound, z, -1e30)
            stay = jnp.maximum(z, lax.log2(1.0 + jnp.exp2(jnp.minimum(z, 126.0))))
            ub[buf, g] = z - stay
            sb[buf, g] = stay.astype(bf16)

    def second(k, buf):
        cells = [cell(k, g) for g in range(group)]
        before = [carry[slot] for slot, _, _ in cells]
        for g, (slot, chunk, _) in enumerate(cells):
            sums = jnp.dot(sb[buf, g], tri_ref[...], preferred_element_type=f32)
            late = sums[:, 128:]
            w = jnp.concatenate(
                [
                    jnp.exp2(ub[buf, g, :, :128] - sums[:, :128] - before[g]).astype(bf16),
                    jnp.exp2(ub[buf, g, :, 128:] - jnp.where(last, 0.0, late) - before[g]).astype(bf16),
                ],
                axis=1,
            )
            carry[slot] = before[g] + jnp.broadcast_to(late[:, 127:128], (256, 128))
            vx = kv_ref[chunk, 80:144, :]
            v = jnp.concatenate([vx[:, :128], vx[:, 128:]], axis=0)
            zero = jnp.zeros_like(v)
            both = jnp.concatenate([jnp.where(lane < 64, v, zero), jnp.where(lane < 64, zero, v)], axis=0)
            acc[slot] += jnp.dot(w, both, preferred_element_type=f32)

    first(0, 0)

    def step(j, _):
        first(2 * j + 1, 1)
        second(2 * j, 0)
        first(2 * j + 2, 0)
        second(2 * j + 1, 1)
        return 0

    lax.fori_loop(0, tab[sp, 0], step, 0)

    def finish(s, _):
        for p in range(4):
            pair = []
            for h in (2 * p, 2 * p + 1):
                a = acc[s, pl.ds(h * 32, 32), :]
                pair.append(a[:, :64] + a[:, 64:])
            out_ref[pl.ds(s * 32, 32), pl.ds(128 * p, 128)] = jnp.concatenate(pair, axis=1).astype(bf16)
        return 0

    lax.fori_loop(0, nt, finish, 0)


def triangle():
    t = np.tril(np.ones((256, 256), np.float32), -1)
    t[:, 255] = 1.0
    return t


def attend(tab, queries, more, kv, group):
    nt = (queries.shape[0] + more.shape[0]) // 32
    vm = pl.BlockSpec(memory_space=pltpu.VMEM)
    tile = pltpu.VMEM((nt + 1, 256, 128), jnp.float32)
    return pl.pallas_call(
        functools.partial(attend_kernel, group),
        out_shape=jax.ShapeDtypeStruct((nt * 32, queries.shape[1]), jnp.bfloat16),
        in_specs=[pl.BlockSpec(memory_space=pltpu.SMEM), vm, vm, vm, vm],
        out_specs=vm,
        scratch_shapes=[
            pltpu.VMEM((nt + 1, 256, 256), jnp.bfloat16),
            tile,
            tile,
            pltpu.VMEM((256, 256), jnp.int32),
            pltpu.VMEM((2, group, 256, 256), jnp.float32),
            pltpu.VMEM((2, group, 256, 256), jnp.bfloat16),
        ],
        compiler_params=pltpu.CompilerParams(vmem_limit_bytes=28 * 1024 * 1024),
        cost_estimate=pl.CostEstimate(flops=2 * 10**10, bytes_accessed=3 * 10**6, transcendentals=2 * 10**7),
        name="attend",
    )(tab, queries, more, kv, jnp.asarray(triangle(), jnp.bfloat16))


MESH = pl.DeviceIdType.MESH
VM = pl.BlockSpec(memory_space=pltpu.VMEM)


def place():
    sp, x = lax.axis_index("sp"), lax.axis_index("tp")
    return sp // 8, (sp // 2) % 4, sp % 2, x


def given_tiles(sp, thresholds):
    low = jnp.minimum(sp, 31 - sp)
    n = jnp.int32(0)
    for t in thresholds:
        n = n + jnp.where(low < t, 1, 0)
    return n


def pack_kernel(kv_ref, bias_ref, out_ref):
    f32, bf16 = jnp.float32, jnp.bfloat16
    kv = kv_ref[...].astype(f32)
    keys = kv.T[0:64].astype(bf16)
    shift = bias_ref[...].astype(f32)
    shifts = jnp.concatenate([shift, shift], axis=0).astype(bf16)
    v = kv[:, 64:]
    left = jnp.concatenate([v[0:64], v[128:192]], axis=1)
    right = jnp.concatenate([v[64:128], v[192:256]], axis=1)
    out_ref[0:64, :] = keys
    out_ref[64:80, :] = shifts
    out_ref[80:144, :] = jnp.concatenate([left, right], axis=1).astype(bf16)


def pack(key_value, bias):
    return pl.pallas_call(
        pack_kernel,
        out_shape=jax.ShapeDtypeStruct((144, 256), jnp.bfloat16),
        in_specs=[VM, VM],
        out_specs=VM,
        compiler_params=pltpu.CompilerParams(vmem_limit_bytes=8 * 1024 * 1024),
        cost_estimate=pl.CostEstimate(flops=10**8, bytes_accessed=10**5, transcendentals=0),
        name="pack",
    )(key_value, bias.T)


def gather_kernel(mine_ref, q_ref, kv_ref, theirs_ref, send, recv_a, recv_b, recv_s, q_send, q_recv, local):
    z, y, c, x = place()
    sp = (z * 4 + y) * 2 + c

    def at(zz, yy, cc):
        return (zz % 4 * 4 + yy % 4) * 2 + cc

    barrier = pltpu.get_barrier_semaphore()
    for d in (1, 2, 3):
        pl.semaphore_signal(barrier, inc=1, device_id=(at(z + d, y, c), x), device_id_type=MESH)
        pl.semaphore_signal(barrier, inc=1, device_id=(at(z, y + d, c), x), device_id_type=MESH)
    pl.semaphore_signal(barrier, inc=1, device_id=(at(z, y, 1 - c), x), device_id_type=MESH)
    pl.semaphore_signal(barrier, inc=1, device_id=(31 - sp, x), device_id_type=MESH)
    own = pltpu.make_async_copy(mine_ref, kv_ref.at[sp], local)
    own.start()
    pl.semaphore_wait(barrier, 8)
    sends = []

    def push(src, dst, recv, device):
        copy = pltpu.make_async_remote_copy(
            src_ref=src, dst_ref=dst, send_sem=send.at[len(sends)], recv_sem=recv, device_id=(device, x), device_id_type=MESH
        )
        copy.start()
        sends.append(copy)

    def part_a(ref, block=None):
        return ref.at[pl.ds(0, 80), :] if block is None else ref.at[block, pl.ds(0, 80), :]

    def part_b(ref, block=None):
        return ref.at[pl.ds(80, 64), :] if block is None else ref.at[block, pl.ds(80, 64), :]

    for d in (1, 3, 2):
        push(part_a(mine_ref), part_a(kv_ref, sp), recv_a.at[d, 0], at(z + d, y, c))
        push(part_b(mine_ref), part_b(kv_ref, sp), recv_b.at[0, d], at(z, y + d, c))
    for d in (1, 3, 2):
        push(part_a(mine_ref), part_a(kv_ref, sp), recv_a.at[0, d], at(z, y + d, c))
        push(part_b(mine_ref), part_b(kv_ref, sp), recv_b.at[d, 0], at(z + d, y, c))
    push(part_a(mine_ref), part_a(kv_ref, sp), recv_s.at[0, 0, 0], at(z, y, 1 - c))
    push(part_b(mine_ref), part_b(kv_ref, sp), recv_s.at[0, 0, 1], at(z, y, 1 - c))
    theirs = pltpu.make_async_remote_copy(
        src_ref=q_ref.at[pl.ds(0, 128), :], dst_ref=theirs_ref, send_sem=q_send, recv_sem=q_recv, device_id=(31 - sp, x), device_id_type=MESH
    )

    @pl.when(sp >= 16)
    def _():
        theirs.start()

    def landed(dz, dy, which):
        block = at(z - dz, y - dy, c)
        ref = part_a(kv_ref, block) if which == 0 else part_b(kv_ref, block)
        sem = (recv_a if which == 0 else recv_b).at[dz, dy]
        pltpu.make_async_copy(ref, ref, sem).wait()
        return ref

    for d in (1, 3, 2):
        ref = landed(d, 0, 0)
        for e in (1, 3, 2):
            push(ref, ref, recv_a.at[d, e], at(z, y + e, c))
        push(ref, ref, recv_s.at[d, 0, 0], at(z, y, 1 - c))
        ref = landed(0, d, 1)
        for e in (1, 3, 2):
            push(ref, ref, recv_b.at[e, d], at(z + e, y, c))
        push(ref, ref, recv_s.at[0, d, 1], at(z, y, 1 - c))
    for d in (1, 3, 2):
        ref = landed(0, d, 0)
        push(ref, ref, recv_s.at[0, d, 0], at(z, y, 1 - c))
        ref = landed(d, 0, 1)
        push(ref, ref, recv_s.at[d, 0, 1], at(z, y, 1 - c))
    for d in (1, 3, 2):
        for e in (1, 3, 2):
            ref = landed(d, e, 0)
            push(ref, ref, recv_s.at[d, e, 0], at(z, y, 1 - c))
            ref = landed(e, d, 1)
            push(ref, ref, recv_s.at[e, d, 1], at(z, y, 1 - c))
    for dz in range(4):
        for dy in range(4):
            block = at(z - dz, y - dy, 1 - c)
            for which in (0, 1):
                ref = part_a(kv_ref, block) if which == 0 else part_b(kv_ref, block)
                pltpu.make_async_copy(ref, ref, recv_s.at[dz, dy, which]).wait()
    own.wait()
    for copy in sends:
        copy.wait_send()

    @pl.when(sp >= 16)
    def _():
        theirs.wait_send()

    @pl.when(sp < 16)
    def _():
        theirs.wait_recv()


def gather(mine, queries):
    return pl.pallas_call(
        gather_kernel,
        out_shape=(jax.ShapeDtypeStruct((32, 144, 256), jnp.bfloat16), jax.ShapeDtypeStruct((128, 512), jnp.bfloat16)),
        in_specs=[VM, VM],
        out_specs=(VM, VM),
        scratch_shapes=[
            pltpu.SemaphoreType.DMA((64,)),
            pltpu.SemaphoreType.DMA((4, 4)),
            pltpu.SemaphoreType.DMA((4, 4)),
            pltpu.SemaphoreType.DMA((4, 4, 2)),
            pltpu.SemaphoreType.DMA,
            pltpu.SemaphoreType.DMA,
            pltpu.SemaphoreType.DMA,
        ],
        compiler_params=pltpu.CompilerParams(collective_id=0, has_side_effects=True, vmem_limit_bytes=16 * 1024 * 1024),
        cost_estimate=pl.CostEstimate(flops=10**10, bytes_accessed=3 * 10**6, transcendentals=0),
        name="gather",
    )(mine, queries)


def offsets():
    every = [(dz, dy, dx, dc) for dz in range(4) for dy in range(4) for dx in range(4) for dc in range(2)][1:]
    order = np.random.default_rng(1).permutation(len(every))
    return [every[k] for k in order]


def slot_codes(shape, dim):
    at = lax.broadcasted_iota(jnp.int32, shape, dim)
    return at // 8, at // 4 % 2, at % 4


GROUPS = 4


def layer_kernel(
    thresholds, att_ref, w_hbm, stream_ref, gain_ref, routes_ref, score_ref, sg_hbm, su_hbm, sd_hbm, g_hbm, u_hbm, d_hbm,
    out_ref, w_ref, sg_ref, su_ref, sd_ref, g_ref, u_ref, d_ref, heads, leaving, arrived, done, back,
    load, swap_send, swap_recv, go_send, go_recv, back_send, back_recv,
):
    f32, bf16 = jnp.float32, jnp.bfloat16
    dot = functools.partial(jnp.dot, preferred_element_type=f32)
    z, y, c, x = place()
    sp = (z * 4 + y) * 2 + c
    me = sp * 4 + x
    other = 31 - sp
    n = given_tiles(sp, thresholds)
    low = sp < 16
    steps = offsets()

    def peer(o, way=1):
        return (((z + way * o[0]) % 4 * 4 + (y + way * o[1]) % 4) * 2 + (c + o[3]) % 2, (x + way * o[2]) % 4)

    barrier = pltpu.get_barrier_semaphore()
    for o in steps:
        pl.semaphore_signal(barrier, inc=1, device_id=peer(o), device_id_type=MESH)
    loads = []
    for k, (src, dst) in enumerate(
        ((w_hbm, w_ref), (sg_hbm, sg_ref), (su_hbm, su_ref), (sd_hbm, sd_ref), (g_hbm, g_ref), (u_hbm, u_ref), (d_hbm, d_ref))
    ):
        loads.append(pltpu.make_async_copy(src, dst, load.at[k]))
        loads[-1].start()
    pl.semaphore_wait(barrier, len(steps))

    def tile(s):
        return att_ref.at[pl.ds(s * 32, 32), :]

    def spot(t, half):
        return heads.at[t, pl.ds(half * 32, 32), :]

    jobs = []
    for d in (1, 3, 2, 0):
        for half in (0, 1):
            s = (x + d) % 4 * 2 + half
            made = jnp.logical_or(low, s >= n)
            if d == 0:
                copy = pltpu.make_async_copy(tile(s), spot(x, half), swap_recv.at[x * 2 + half])
            else:
                copy = pltpu.make_async_remote_copy(
                    src_ref=tile(s), dst_ref=spot(x, half), send_sem=swap_send.at[d * 2 + half], recv_sem=swap_recv.at[x * 2 + half],
                    device_id=(sp, (x + d) % 4), device_id_type=MESH,
                )
            jobs.append((made, copy, d != 0))
    for s in range(len(thresholds)):
        made = jnp.logical_and(low, s < n)
        copy = pltpu.make_async_remote_copy(
            src_ref=tile(8 + s), dst_ref=spot(x, s % 2), send_sem=swap_send.at[8 + s], recv_sem=swap_recv.at[x * 2 + s % 2],
            device_id=(other, s // 2), device_id_type=MESH,
        )
        jobs.append((made, copy, True))
    for made, copy, _ in jobs:
        pl.when(made)(copy.start)

    expert = lax.broadcasted_iota(jnp.int32, (128, 64), 0)
    named = jnp.zeros((128, 64), f32)
    for k in range(4):
        named = jnp.where(routes_ref[pl.ds(k, 1), :] == expert, 1.0, named)
    earlier = lax.broadcasted_iota(jnp.int32, (64, 64), 0) < lax.broadcasted_iota(jnp.int32, (64, 64), 1)
    rank = dot(named.astype(bf16), earlier.astype(f32).astype(bf16))
    e, _, _ = slot_codes((1024, 128), 0)
    spread = (e == lax.broadcasted_iota(jnp.int32, (1024, 128), 1)).astype(f32).astype(bf16)
    both = dot(spread, jnp.concatenate([named, rank], axis=1).astype(bf16))
    _, h, k = slot_codes((1024, 64), 0)
    taken = jnp.where(both[:, 64:] == k.astype(f32), both[:, :64], 0.0)
    pick = jnp.concatenate([jnp.where(h == 0, taken, 0.0), jnp.where(h == 1, taken, 0.0)], axis=1).astype(bf16)

    loads[0].wait()
    for t in range(4):
        for half in (0, 1):
            pltpu.make_async_copy(spot(t, half), spot(t, half), swap_recv.at[t * 2 + half]).wait()
    mixed = sum(dot(heads[t], w_ref[pl.ds(512 * t, 512), :]) for t in range(4))
    resid = (stream_ref[...].astype(f32) + mixed).astype(bf16).astype(f32)
    factor = lax.rsqrt(jnp.mean(resid * resid, axis=1, keepdims=True) + 1e-06)
    normed = (resid * factor * gain_ref[...]).astype(bf16)
    picked = dot(pick, jnp.concatenate([normed[:, :1024], normed[:, 1024:]], axis=0))
    leaving[...] = picked.reshape(128, 8, 1024).astype(bf16)

    size = 128 // GROUPS
    places = list(range(len(steps) + 1))
    for j, o in enumerate(steps):
        s, t = peer(o)
        pltpu.make_async_remote_copy(
            src_ref=leaving.at[s * 4 + t], dst_ref=arrived.at[j], send_sem=go_send, recv_sem=go_recv.at[j // size],
            device_id=(s, t), device_id_type=MESH,
        ).start()
    pltpu.make_async_copy(leaving.at[me], arrived.at[127], go_recv.at[GROUPS - 1]).start()

    for k in (1, 2, 3):
        loads[k].wait()
    lit = dot(normed, sg_ref[...])
    inner = (lit * jax.nn.sigmoid(lit) * dot(normed, su_ref[...])).astype(bf16)
    base = resid + dot(inner, sd_ref[...])
    score = score_ref[...]
    gates = 2.5 * score / jnp.sum(score, axis=0, keepdims=True)
    gate = jnp.zeros((128, 64), f32)
    for k in range(4):
        gate = jnp.where(routes_ref[pl.ds(k, 1), :] == expert, gates[k : k + 1, :], gate)
    turned = jnp.concatenate([rank, gate], axis=1).T
    rank, gate = turned[0:64], turned[64:128]
    high = gate.astype(bf16)
    small = (gate - high.astype(f32)).astype(bf16)
    e, _, _ = slot_codes((128, 1024), 1)
    spread = (e == lax.broadcasted_iota(jnp.int32, (128, 1024), 0)).astype(f32).astype(bf16)
    wide = dot(jnp.concatenate([rank.astype(bf16), high, small], axis=0), spread)
    _, h, k = slot_codes((64, 1024), 1)
    mine = wide[0:64] == k.astype(f32)
    parts = []
    for half in (0, 1):
        for piece in (wide[64:128], wide[128:192]):
            parts.append(jnp.where(mine & (h == half), piece, 0.0))
    weigh = jnp.concatenate(parts, axis=0).astype(bf16)

    for k in (4, 5, 6):
        loads[k].wait()
    top = lax.broadcasted_iota(jnp.int32, (size // 2, 8, 1024), 1) < 4
    for q in range(GROUPS):
        rows = pl.ds(q * size, size)
        pltpu.make_async_copy(arrived.at[rows], arrived.at[rows], go_recv.at[q]).wait()
        wide = arrived[rows].astype(f32).reshape(size // 2, 2, 8, 1024)
        a, b = wide[:, 0], wide[:, 1]
        left = jnp.where(top, a, pltpu.roll(b, 4, 1)).reshape(size * 4, 1024).astype(bf16)
        right = jnp.where(top, pltpu.roll(a, 4, 1), b).reshape(size * 4, 1024).astype(bf16)
        gate = dot(left, g_ref[0:1024, :]) + dot(right, g_ref[1024:2048, :])
        up = dot(left, u_ref[0:1024, :]) + dot(right, u_ref[1024:2048, :])
        inner = (gate * jax.nn.sigmoid(gate) * up).astype(bf16)
        lo = dot(inner, d_ref[:, 0:1024]).reshape(size // 2, 8, 1024)
        hi = dot(inner, d_ref[:, 1024:2048]).reshape(size // 2, 8, 1024)
        first = jnp.where(top, lo, pltpu.roll(hi, 4, 1))
        second = jnp.where(top, pltpu.roll(lo, 4, 1), hi)
        done[rows] = jnp.stack([first, second], axis=1).reshape(size, 8, 1024).astype(bf16)
        for j in range(q * size, (q + 1) * size):
            if j < len(steps):
                s, t = peer(steps[j], -1)
                pltpu.make_async_remote_copy(
                    src_ref=done.at[j], dst_ref=back.at[me], send_sem=back_send, recv_sem=back_recv,
                    device_id=(s, t), device_id_type=MESH,
                ).start()
            else:
                pltpu.make_async_copy(done.at[j], back.at[me], back_recv).start()

    pltpu.make_async_copy(back, back, back_recv).wait()
    total = dot(weigh, back[...].reshape(1024, 1024))
    out_ref[:, 0:1024] = (base[:, 0:1024] + total[0:64] + total[64:128]).astype(bf16)
    out_ref[:, 1024:2048] = (base[:, 1024:2048] + total[128:192] + total[192:256]).astype(bf16)
    for made, copy, remote in jobs:
        if remote:
            pl.when(made)(copy.wait_send)
    count = pl.ds(0, len(steps))
    pltpu.make_async_copy(leaving.at[count], arrived.at[count], go_send).wait()
    pltpu.make_async_copy(done.at[count], back.at[count], back_send).wait()


def layer(att, thresholds, w, stream, gain, routes, score, sg, su, sd, g, u, d):
    bf16 = jnp.bfloat16
    hbm = pl.BlockSpec(memory_space=pltpu.HBM)
    chunk = pltpu.VMEM((128, 8, 1024), bf16)
    dma = pltpu.SemaphoreType.DMA
    return pl.pallas_call(
        functools.partial(layer_kernel, thresholds),
        out_shape=jax.ShapeDtypeStruct(stream.shape, bf16),
        in_specs=[VM, hbm, VM, VM, VM, VM, hbm, hbm, hbm, hbm, hbm, hbm],
        out_specs=VM,
        scratch_shapes=[pltpu.VMEM(a.shape, bf16) for a in (w, sg, su, sd, g, u, d)]
        + [pltpu.VMEM((4, 64, 512), bf16), chunk, chunk, chunk, chunk]
        + [dma((7,)), dma((12,)), dma((8,)), dma, dma((GROUPS,)), dma, dma],
        compiler_params=pltpu.CompilerParams(collective_id=1, has_side_effects=True, vmem_limit_bytes=46 * 1024 * 1024),
        cost_estimate=pl.CostEstimate(flops=4 * 10**10, bytes_accessed=3 * 10**7, transcendentals=0),
        name="layer",
    )(att, w, stream, gain, routes.T, score.T, sg, su, sd, g, u, d)


def body(
    queries, key_value, break_bias, stream, out_proj, ffn_gain, routes, route_score,
    expert_gate, expert_up, expert_down, shared_gate, shared_up, shared_down,
):
    table, give = schedule(lax.axis_size("sp"), queries.shape[0] // 32, GROUP)
    thresholds = tuple(int((give >= k).sum()) for k in range(1, int(give.max()) + 1))
    kv, theirs = gather(pack(key_value[:, 0, :], break_bias), queries)
    made = attend(jnp.asarray(table), queries, theirs, kv, GROUP)
    return layer(
        made, thresholds, out_proj, stream, ffn_gain.reshape(1, -1), routes, route_score,
        shared_gate, shared_up, shared_down, expert_gate[0], expert_up[0], expert_down[0],
    )


def solution(mesh):
    return jax.shard_map(
        body,
        mesh=mesh,
        in_specs=(
            P("sp", "tp"),
            P("sp", "tp", None),
            P("sp", "tp"),
            P(("sp", "tp"), None),
            P(),
            P(),
            P(("sp", "tp"), None),
            P(("sp", "tp"), None),
            P(("sp", "tp"), None, None),
            P(("sp", "tp"), None, None),
            P(("sp", "tp"), None, None),
            P(),
            P(),
            P(),
        ),
        out_specs=P(("sp", "tp"), None),
        check_vma=False,
    )
```
